32 devices in a mesh: ep: 8 (over z, x), tp: 4 (over y, core).
Axes of the slice: x: 2, y: 2, z: 4, core: 2. Of those that a mesh axis runs over, the one named last changes fastest.
Arguments:
- hidden: bfloat16 [32, 2048], P('ep'), may hold values from -6 to 6
- attn_gain: float32 [2048], replicated, may hold values from 0.3 to 3
- query_weight: bfloat16 [2048, 2048], P('ep', 'tp'), may hold values from -0.125 to 0.125
- head_bias: float32 [16], replicated, may hold values from -10 to -4
- key_cache: bfloat16 [32, 4, 1024, 128], P('ep', 'tp'), may hold values from -6 to 6
- value_cache: bfloat16 [32, 4, 1024, 128], P('ep', 'tp'), may hold values from -7 to 7
- lengths: int32 [32], P('ep'), may hold values from 256 to 1024, as said below
- out_weight: bfloat16 [2048, 2048], P('tp', 'ep'), may hold values from -0.125 to 0.125
- moe_gain: float32 [2048], replicated, may hold values from 0.1 to 1.9
- route_group: int32 [32], P('ep'), may hold values from 0 to 1, as said below
- route_inner: int32 [32, 2], P('ep'), may hold values from 0 to 3, as said below
- route_weight: bfloat16 [32, 2], P('ep'), may hold values from 0.25 to 1
- gate_w: bfloat16 [8, 2048, 768], P('ep', None, 'tp'), may hold values from -0.125 to 0.125
- up_w: bfloat16 [8, 2048, 768], P('ep', None, 'tp'), may hold values from -0.125 to 0.125
- down_w: bfloat16 [8, 768, 2048], P('ep', 'tp'), may hold values from -0.21875 to 0.21875
Outputs:
- mixed: bfloat16 [32, 2048], P('ep', 'tp')
The draws below stay inside these ranges and needn't reach their ends.
Inputs may be any that keep to these rules, and one draw needn't show every extreme that they name: `lengths`: some sequence has length 1024 in every draw. Within the rows of one device (aligned blocks of 4 rows) no expert route_group * 4 + route_inner is named twice; one expert is named in every block. `route_inner`: the 2 entries of a row differ.
All inputs are finite; a program needn't handle non-finite values.
Results may differ from the reference program's by a relative error of at most 0.013.
Values may be sent and summed in bfloat16 or wider, within the bound.
A program may use at most 64 MiB of HBM per device.

```python
import math
import jax
import jax.numpy as jnp
from jax import lax

D = 2048
HEADS = 16
KV_HEADS = 4
HEAD_SIZE = 128
FF_EXP = 768
TOPK = 2
SEQ_DEV = 4
CACHE = 1024
TOKENS = 32
EXPERTS = 8
GROUPS = 2
GROUP_SIZE = 4
N_EP = 8
N_TP = 4


def routing_tables(key):
    base = jax.random.fold_in(key, 7001)
    key_hot, key_perm, key_pairs, key_star = jax.random.split(base, 4)
    blocks = TOKENS // SEQ_DEV
    pairs_total = EXPERTS // TOPK
    pairs_group = GROUP_SIZE // TOPK
    hottest = jax.random.randint(key_hot, (), 0, EXPERTS)
    hot_group = hottest // GROUP_SIZE
    hot_inner = hottest % GROUP_SIZE
    perm_keys = jax.random.split(key_perm, blocks * GROUPS)
    perms = jax.vmap(lambda one_key: jax.random.permutation(one_key, GROUP_SIZE))(perm_keys)
    perms = perms.reshape(blocks, GROUPS, GROUP_SIZE)
    hot_perm = perms[:, hot_group, :]
    hot_place = jnp.argmax((hot_perm == hot_inner).astype(jnp.int32), axis=1)
    hot_pair = hot_group * pairs_group + hot_place // TOPK
    pair_keys = jax.random.split(key_pairs, blocks)
    order = jax.vmap(lambda one_key: jax.random.permutation(one_key, pairs_total))(pair_keys)
    hot_pos = jnp.argmax((order == hot_pair[:, None]).astype(jnp.int32), axis=1)
    starred = jax.random.randint(key_star, (blocks,), 0, SEQ_DEV)
    at_star = jnp.take_along_axis(order, starred[:, None], axis=1)[:, 0]
    places = jnp.arange(pairs_total)[None, :]
    order = jnp.where(places == starred[:, None], hot_pair[:, None], jnp.where(places == hot_pos[:, None], at_star[:, None], order))
    picked = order[:, :SEQ_DEV]
    groups = picked // pairs_group
    within = picked % pairs_group
    slot_index = within[:, :, None] * TOPK + jnp.arange(TOPK)[None, None, :]
    own_perm = perms[jnp.arange(blocks)[:, None], groups]
    inner = jnp.take_along_axis(own_perm, slot_index, axis=2)
    return (groups.reshape(TOKENS).astype(jnp.int32), inner.reshape(TOKENS, TOPK).astype(jnp.int32))


def draw_route_group(key, part):
    return routing_tables(key)[0]


def draw_route_inner(key, part):
    return routing_tables(key)[1]


def draw_lengths(key, part):
    base = jax.random.fold_in(key, 7101)
    key_len, key_top = jax.random.split(base, 2)
    spans = jax.random.randint(key_len, (TOKENS,), CACHE // 4, CACHE + 1)
    longest = jax.random.randint(key_top, (), 0, TOKENS)
    return jnp.where(jnp.arange(TOKENS) == longest, CACHE, spans).astype(jnp.int32)


def draw_head_bias(key, part):
    base = jax.random.fold_in(key, 7201)
    values = jax.random.uniform(base, (HEADS,), jnp.float32, -10.0, -4.0)
    return values


def draw_value_cache(key, part):
    base = jax.random.fold_in(key, 7301)
    key_common, key_noise = jax.random.split(base, 2)
    common = jax.random.normal(key_common, (TOKENS, KV_HEADS, 1, HEAD_SIZE), jnp.float32)
    noise = jax.random.normal(key_noise, (TOKENS, KV_HEADS, CACHE, HEAD_SIZE), jnp.float32)
    values = common + noise
    return jnp.clip(values, -7.0, 7.0).astype(jnp.bfloat16)


def levels(rng, dims, pieces, smallest, largest):
    level, own = 1.0, jax.random.fold_in(rng, 6)
    for position, parts in pieces:
        draws = jnp.exp(jax.random.uniform(jax.random.fold_in(own, position), (parts,), jnp.float32, smallest / len(pieces), largest / len(pieces)))
        level = level * jnp.repeat(draws, dims[position] // parts).reshape([-1 if axis == position else 1 for axis in range(len(dims))])
    return level


def centred(rng, dims, deviation, most, pieces=(), held_as=jnp.bfloat16):
    drawn = jax.random.normal(rng, dims, jnp.float32) * deviation
    if len(pieces) > 0:
        drawn = levels(rng, dims, pieces, -0.22, 0.18) * drawn
    return jnp.clip(drawn, min=-most, max=most).astype(held_as)


def setup_inputs(seed: int = 0) -> dict:
    streams_of = jax.random.split(jax.random.key(seed), 16)
    return {
        "hidden": centred(streams_of[0], (TOKENS, D), 1.0, 6.0, ((0, 8),)),
        "attn_gain": jnp.clip(jnp.exp(jax.random.uniform(streams_of[1], (D,), jnp.float32, math.log(0.3), math.log(3.0))), 0.3, 3.0),
        "query_weight": centred(streams_of[2], (D, HEADS * HEAD_SIZE), D ** -0.5, 0.125, ((0, 8), (1, 4))),
        "head_bias": draw_head_bias(jax.random.fold_in(streams_of[15], 71), 0),
        "key_cache": centred(streams_of[4], (TOKENS, KV_HEADS, CACHE, HEAD_SIZE), 1.0, 6.0, ((0, 8), (1, 4))),
        "value_cache": draw_value_cache(jax.random.fold_in(streams_of[15], 71), 0),
        "lengths": draw_lengths(jax.random.fold_in(streams_of[15], 71), 0),
        "out_weight": centred(streams_of[7], (HEADS * HEAD_SIZE, D), (HEADS * HEAD_SIZE) ** -0.5, 0.125, ((0, 4), (1, 8))),
        "moe_gain": jnp.clip(1.0 + 0.18 * jax.random.normal(streams_of[8], (D,), jnp.float32), 0.1, 1.9),
        "route_group": draw_route_group(jax.random.fold_in(streams_of[15], 71), 0),
        "route_inner": draw_route_inner(jax.random.fold_in(streams_of[15], 71), 0),
        "route_weight": jnp.clip(0.25 + 0.75 * jax.random.uniform(streams_of[11], (TOKENS, TOPK), jnp.float32) ** levels(streams_of[11], (TOKENS, TOPK), ((0, 8),), -0.2, 0.2), 0.25, 1.0).astype(jnp.bfloat16),
        "gate_w": centred(streams_of[12], (EXPERTS, D, FF_EXP), D ** -0.5, 0.125, ((0, 8), (2, 4))),
        "up_w": centred(streams_of[13], (EXPERTS, D, FF_EXP), D ** -0.5, 0.125, ((0, 8), (2, 4))),
        "down_w": centred(streams_of[14], (EXPERTS, FF_EXP, D), FF_EXP ** -0.5, 0.21875, ((0, 8), (1, 4))),
    }


rms_epsilon = 1e-06

def rms_scale(values, gain):
    wide = values.astype(jnp.float32)
    scaled = wide * lax.rsqrt(lax.optimization_barrier(jnp.mean(wide * wide, axis=-1, keepdims=True)) + rms_epsilon)
    return (scaled * gain).astype(jnp.bfloat16)

def attend(queries, key_cache, value_cache, lengths, head_bias):
    group_heads = HEADS // KV_HEADS
    bias_grid = head_bias.reshape(KV_HEADS, group_heads)

    def one_sequence(args):
        query_row, keys, values, length = args
        grouped = query_row.reshape(KV_HEADS, group_heads, HEAD_SIZE).astype(jnp.float32)
        scores = jnp.einsum('kgd,kpd->kgp', grouped, keys.astype(jnp.float32)) * HEAD_SIZE ** (-0.5)
        scores = scores + bias_grid[:, :, None]
        visible = jnp.arange(CACHE, dtype=jnp.int32) < length
        log_keep = jnp.where(visible[None, None, :], jax.nn.log_sigmoid(-scores), 0.0)
        later_sum = lax.cumsum(log_keep, axis=2, reverse=True) - log_keep
        weight = jnp.where(visible[None, None, :], jnp.exp(jax.nn.log_sigmoid(scores) + later_sum), 0.0)
        weight = weight.astype(jnp.bfloat16)
        result = jnp.einsum('kgp,kpd->kgd', weight.astype(jnp.float32), values.astype(jnp.float32))
        return result.astype(jnp.bfloat16).reshape(HEADS, HEAD_SIZE)
    return lax.map(one_sequence, (queries, key_cache, value_cache, lengths))

def reference(hidden, attn_gain, query_weight, head_bias, key_cache, value_cache, lengths, out_weight, moe_gain, route_group, route_inner, route_weight, gate_w, up_w, down_w):
    normed = rms_scale(hidden, attn_gain)
    queries = jnp.dot(normed, query_weight, preferred_element_type=jnp.float32).astype(jnp.bfloat16)
    queries = queries.reshape(TOKENS, HEADS, HEAD_SIZE)
    heads_out = attend(queries, key_cache, value_cache, lengths, head_bias).reshape(TOKENS, HEADS * HEAD_SIZE)
    head_width = HEADS * HEAD_SIZE // N_TP
    attended = jnp.zeros((TOKENS, D), jnp.float32)
    for group in range(N_TP):
        partial_value = jnp.dot(heads_out[:, group * head_width:(group + 1) * head_width], out_weight[group * head_width:(group + 1) * head_width], preferred_element_type=jnp.float32)
        attended = attended + lax.optimization_barrier(partial_value.astype(jnp.bfloat16)).astype(jnp.float32)
    residual = (hidden.astype(jnp.float32) + attended).astype(jnp.bfloat16)
    normed_two = rms_scale(residual, moe_gain)
    assigned = TOKENS * TOPK
    chosen = (route_group[:, None] * GROUP_SIZE + route_inner).reshape(assigned).astype(jnp.int32)
    padded_rows = jnp.concatenate([normed_two, jnp.zeros((1, D), jnp.bfloat16)], axis=0)
    weights_flat = jnp.concatenate([route_weight.reshape(assigned).astype(jnp.float32), jnp.zeros((1,), jnp.float32)], axis=0)
    ff_width = FF_EXP // N_TP

    def one_expert(expert):
        slots = jnp.nonzero(chosen == expert, size=N_EP, fill_value=assigned)[0].astype(jnp.int32)
        rows = padded_rows[slots // TOPK]
        gate_all = gate_w[expert]
        up_all = up_w[expert]
        down_all = down_w[expert]
        total = jnp.zeros((N_EP, D), jnp.float32)
        for group in range(N_TP):
            gated = jnp.dot(rows, gate_all[:, group * ff_width:(group + 1) * ff_width], preferred_element_type=jnp.float32)
            upped = jnp.dot(rows, up_all[:, group * ff_width:(group + 1) * ff_width], preferred_element_type=jnp.float32)
            activated = (jax.nn.silu(gated) * upped).astype(jnp.bfloat16)
            down_part = jnp.dot(activated, down_all[group * ff_width:(group + 1) * ff_width], preferred_element_type=jnp.float32)
            total = total + lax.optimization_barrier(down_part.astype(jnp.bfloat16)).astype(jnp.float32)
        return (slots, total.astype(jnp.bfloat16))
    slots, outputs = lax.map(one_expert, jnp.arange(EXPERTS, dtype=jnp.int32))
    contrib = weights_flat[slots][:, :, None] * outputs.astype(jnp.float32)
    collected = jnp.zeros((assigned + 1, D), jnp.float32).at[slots.reshape(-1)].add(contrib.reshape(-1, D))
    routed = lax.optimization_barrier(jnp.sum(collected[:assigned].reshape(TOKENS, TOPK, D), axis=1))
    return (residual.astype(jnp.float32) + routed).astype(jnp.bfloat16)
```

```python
import functools

import jax
import jax.numpy as jnp
from jax import lax
from jax.experimental import pallas as pl
from jax.experimental.pallas import tpu as pltpu
from jax.sharding import PartitionSpec as P

rms_epsilon = 1e-06


def rms_scale(values, gain):
    wide = values.astype(jnp.float32)
    scaled = wide * lax.rsqrt(jnp.mean(wide * wide, axis=-1, keepdims=True) + rms_epsilon)
    return (scaled * gain).astype(jnp.bfloat16)


def body(
    hidden,
    attn_gain,
    query_weight,
    head_bias,
    key_cache,
    value_cache,
    lengths,
    out_weight,
    moe_gain,
    route_group,
    route_inner,
    route_weight,
    gate_w,
    up_w,
    down_w,
):
    n_tp = lax.axis_size("tp")
    n_ep = lax.axis_size("ep")
    tokens = hidden.shape[0]
    d_model = hidden.shape[1]
    normed = rms_scale(hidden, attn_gain)
    feature_block = lax.all_to_all(normed, "ep", split_axis=1, concat_axis=0, tiled=True)
    queries = lax.psum_scatter(
        jnp.dot(feature_block, query_weight, preferred_element_type=jnp.float32),
        "ep",
        scatter_dimension=0,
        tiled=True,
    ).astype(jnp.bfloat16)
    head_size = key_cache.shape[3]
    local_kv = key_cache.shape[1]
    cache_len = key_cache.shape[2]
    local_heads = queries.shape[1] // head_size
    group_heads = local_heads // local_kv
    queries = queries.reshape(tokens, local_kv, group_heads, head_size)
    own_bias = lax.dynamic_slice_in_dim(
        head_bias, lax.axis_index("tp") * local_heads, local_heads, 0
    )
    own_bias = own_bias.reshape(local_kv, group_heads)
    scores = jnp.einsum(
        "tkgd,tkpd->tkgp", queries, key_cache, preferred_element_type=jnp.float32
    ) * head_size ** (-0.5)
    scores = scores + own_bias[None, :, :, None]
    position = jnp.arange(cache_len, dtype=jnp.int32)
    visible = position[None, None, None, :] < lengths[:, None, None, None]
    log_keep = jnp.where(visible, jax.nn.log_sigmoid(-scores), 0.0)
    later_sum = lax.cumsum(log_keep, axis=3, reverse=True) - log_keep
    weight = jnp.where(visible, jnp.exp(jax.nn.log_sigmoid(scores) + later_sum), 0.0).astype(
        jnp.bfloat16
    )
    heads_out = jnp.einsum(
        "tkgp,tkpd->tkgd", weight, value_cache, preferred_element_type=jnp.float32
    )
    heads_out = heads_out.astype(jnp.bfloat16).reshape(tokens, -1)
    partial_value = jnp.dot(
        heads_out,
        lax.all_gather(out_weight, "ep", axis=1, tiled=True),
        preferred_element_type=jnp.float32,
    )
    rounded = lax.optimization_barrier(partial_value.astype(jnp.bfloat16)).astype(jnp.float32)
    attended = lax.psum(rounded.astype(jnp.bfloat16), "tp").astype(jnp.float32)
    residual = (hidden.astype(jnp.float32) + attended).astype(jnp.bfloat16)
    normed_two = rms_scale(residual, moe_gain)
    per_device = gate_w.shape[0]
    experts = per_device * n_ep
    group_count = max(2, experts // 32)
    group_size = experts // group_count
    chosen = route_group[:, None] * group_size + route_inner
    matches = chosen[:, :, None] == jnp.arange(experts, dtype=jnp.int32)[None, None, :]
    picked = jnp.any(matches, axis=1).astype(jnp.bfloat16)
    mixing = jnp.sum(
        jnp.where(matches, route_weight[:, :, None].astype(jnp.float32), 0.0), axis=1
    ).astype(jnp.bfloat16)
    part_width = d_model // n_tp
    outgoing = jnp.einsum("te,td->ed", picked, normed_two, preferred_element_type=jnp.float32)
    outgoing = outgoing.astype(jnp.bfloat16).reshape(n_ep, per_device, d_model)
    arrived = lax.all_to_all(outgoing, "ep", split_axis=0, concat_axis=0, tiled=True)
    gated_in = jnp.einsum("sed,edf->sef", arrived, gate_w, preferred_element_type=jnp.float32)
    up_proj = jnp.einsum("sed,edf->sef", arrived, up_w, preferred_element_type=jnp.float32)
    activated = (jax.nn.silu(gated_in) * up_proj).astype(jnp.bfloat16)
    down_out = jnp.einsum("sef,efd->sed", activated, down_w, preferred_element_type=jnp.float32)
    down_rounded = lax.optimization_barrier(down_out.astype(jnp.bfloat16)).astype(jnp.float32)
    summed = lax.psum_scatter(
        down_rounded.astype(jnp.bfloat16), "tp", scatter_dimension=2, tiled=True
    )
    returned = lax.all_to_all(summed, "ep", split_axis=0, concat_axis=0, tiled=True).reshape(
        experts, part_width
    )
    routed = jnp.dot(mixing, returned, preferred_element_type=jnp.float32)
    own_residual = lax.dynamic_slice_in_dim(
        residual, lax.axis_index("tp") * part_width, part_width, 1
    )
    return (own_residual.astype(jnp.float32) + routed).astype(jnp.bfloat16)


MESH = pl.DeviceIdType.MESH


def kernel(
    n_ep,
    n_tp,
    group_size,
    head_bias,
    lengths,
    route_group,
    route_inner,
    hidden_hbm,
    attn_gain_hbm,
    query_hbm,
    key_hbm,
    value_hbm,
    out_hbm,
    moe_gain_hbm,
    route_weight_hbm,
    gate_hbm,
    up_hbm,
    down_hbm,
    mixed,
    hidden,
    attn_gain,
    query_w,
    keys,
    values,
    out_w,
    moe_gain,
    route_weight,
    gate_w,
    up_w,
    down_w,
    load_sem,
    x_in,
    r_out,
    r_in,
    q_out,
    q_in,
    h_out,
    h_in,
    a_out,
    a_in,
    m_out,
    m_in,
    z_out,
    z_in,
    x_send,
    x_recv,
    r_send,
    r_recv,
    q_send,
    q_recv,
    h_send,
    h_recv,
    a_send,
    a_recv,
    m_send,
    m_recv,
    z_send,
    z_recv,
    x_all,
    route_all,
    q_rows,
    score_rows,
    weight_rows,
    head_rows,
):
    f32, bf16 = jnp.float32, jnp.bfloat16
    ep = lax.axis_index("ep")
    tp = lax.axis_index("tp")
    tokens, d_model = hidden.shape
    chunk = d_model // n_ep
    total = tokens * n_ep
    cache_len, head_size = keys.shape[1], keys.shape[2]
    heads = query_w.shape[1] // head_size
    rows = tokens * heads
    part = d_model // n_tp
    per_part = part // chunk
    slots = route_inner.shape[1]

    loads = [
        pltpu.make_async_copy(src, dst, load_sem.at[index])
        for index, (src, dst) in enumerate(
            (
                (hidden_hbm, hidden),
                (attn_gain_hbm, attn_gain),
                (query_hbm, query_w),
                (key_hbm.at[:, 0], keys),
                (value_hbm.at[:, 0], values),
                (out_hbm, out_w),
                (moe_gain_hbm, moe_gain),
                (route_weight_hbm, route_weight),
                (gate_hbm.at[0], gate_w),
                (up_hbm.at[0], up_w),
                (down_hbm.at[0], down_w),
            )
        )
    ]
    for load in loads:
        load.start()

    barrier = pltpu.get_barrier_semaphore()
    others = [(i, j) for i in range(n_ep) for j in range(n_tp) if (i, j) != (0, 0)]
    for i, j in others:
        peer = (lax.rem(ep + i, n_ep), lax.rem(tp + j, n_tp))
        pl.semaphore_signal(barrier, inc=1, device_id=peer, device_id_type=MESH)

    lane = lax.broadcasted_iota(jnp.int32, (1, slots * 128), 1)
    own_route = jnp.full((1, slots * 128), -1, jnp.int32)
    chosen = [
        [route_group[i] * group_size + route_inner[i, k] for k in range(slots)]
        for i in range(tokens)
    ]
    for i in range(tokens):
        for k in range(slots):
            own_route = jnp.where(lane == k * 128 + ep * tokens + i, chosen[i][k], own_route)
    r_out[...] = own_route

    pl.semaphore_wait(barrier, len(others))
    loads[0].wait()

    sends = []

    def push(src, dst, peer, send_sem, recv_sem):
        copy = pltpu.make_async_remote_copy(
            src_ref=src,
            dst_ref=dst,
            send_sem=send_sem,
            recv_sem=recv_sem,
            device_id=peer,
            device_id_type=MESH,
        )
        copy.start()
        sends.append(copy)

    def arrived(ref, sem):
        pltpu.make_async_copy(ref, ref, sem).wait()

    def columns(index, width):
        return pl.ds(pl.multiple_of(index * width, 128), width)

    for k in range(1, n_ep):
        to = lax.rem(ep + k, n_ep)
        push(hidden.at[:, columns(to, chunk)], x_in.at[ep], (to, tp), x_send.at[k], x_recv.at[ep])
    pltpu.make_async_copy(hidden.at[:, columns(ep, chunk)], x_in.at[ep], x_recv.at[ep]).start()
    for k in range(1, n_ep):
        to = lax.rem(ep + k, n_ep)
        push(r_out, r_in.at[ep], (to, tp), r_send.at[k], r_recv.at[ep])
    pltpu.make_async_copy(r_out, r_in.at[ep], r_recv.at[ep]).start()

    wide = hidden[...].astype(f32)
    scale = lax.rsqrt(jnp.mean(wide * wide, axis=-1, keepdims=True) + rms_epsilon)

    loads[1].wait()
    loads[2].wait()
    for e in range(n_ep):
        arrived(x_in.at[e], x_recv.at[e])
        x_all[e * tokens : (e + 1) * tokens, :] = x_in[e].astype(f32)
    features = (x_all[...] * attn_gain[:, columns(ep, chunk)]).astype(bf16)
    query_parts = jnp.dot(features, query_w[...], preferred_element_type=f32)
    for e in range(n_ep):
        q_out[e] = query_parts[e * tokens : (e + 1) * tokens, :]
    for k in range(1, n_ep):
        to = lax.rem(ep + k, n_ep)
        push(q_out.at[to], q_in.at[ep], (to, tp), q_send.at[k], q_recv.at[ep])
    pltpu.make_async_copy(q_out.at[ep], q_in.at[ep], q_recv.at[ep]).start()

    for e in range(n_ep):
        arrived(r_in.at[e], r_recv.at[e])
        for k in range(slots):
            route_all[k, e : e + 1, :] = r_in[e, :, k * 128 : (k + 1) * 128]
    tables = [route_all[k] for k in range(slots)]
    picks = []
    for e in range(n_ep):
        hit = tables[0] == e
        for table in tables[1:]:
            hit = hit | (table == e)
        picks.append(jnp.where(hit, 1.0, 0.0))
    pick = jnp.concatenate(picks, axis=0)[:, :total].astype(bf16)

    row = lax.broadcasted_iota(jnp.int32, (rows, 1), 0)
    bias = jnp.zeros((rows, 1), f32)
    length = jnp.zeros((rows, 1), jnp.int32)
    for i in range(tokens):
        length = jnp.where(row // heads == i, lengths[i], length)
    for h in range(heads):
        bias = jnp.where(row % heads == h, head_bias[tp * heads + h], bias)
    above = lax.broadcasted_iota(jnp.int32, (128, 128), 0) > lax.broadcasted_iota(
        jnp.int32, (128, 128), 1
    )
    above = jnp.where(above, 1.0, 0.0).astype(bf16)
    loads[3].wait()

    for e in range(n_ep):
        arrived(q_in.at[e], q_recv.at[e])
    queries = q_in[0]
    for e in range(1, n_ep):
        queries = queries + q_in[e]
    queries = queries * scale
    for i in range(tokens):
        for h in range(heads):
            q_rows[i * heads + h : i * heads + h + 1, :] = queries[
                i : i + 1, h * head_size : (h + 1) * head_size
            ]
    for i in range(tokens):
        score_rows[i * heads : (i + 1) * heads, :] = lax.dot_general(
            q_rows[i * heads : (i + 1) * heads, :].astype(bf16),
            keys[i],
            (((1,), (1,)), ((), ())),
            preferred_element_type=f32,
        )
    blocks = cache_len // 128
    keeps, takes, seen = [], [], []
    position = lax.broadcasted_iota(jnp.int32, (rows, 128), 1)
    for c in range(blocks):
        score = score_rows[:, c * 128 : (c + 1) * 128] * head_size ** (-0.5) + bias
        visible = position + c * 128 < length
        soft = jnp.log1p(jnp.exp(-jnp.abs(score)))
        keeps.append(jnp.where(visible, -jnp.maximum(score, 0.0) - soft, 0.0))
        takes.append(jnp.minimum(score, 0.0) - soft)
        seen.append(visible)
    keep = jnp.concatenate(keeps, axis=0)
    high = keep.astype(bf16)
    rest = keep - high.astype(f32)
    middle = rest.astype(bf16)
    low = (rest - middle.astype(f32)).astype(bf16)
    later = (
        jnp.dot(high, above, preferred_element_type=f32)
        + jnp.dot(middle, above, preferred_element_type=f32)
        + jnp.dot(low, above, preferred_element_type=f32)
    )
    tail = jnp.zeros((rows, 1), f32)
    for c in reversed(range(blocks)):
        exponent = takes[c] + later[c * rows : (c + 1) * rows, :] + tail
        weight_rows[:, c * 128 : (c + 1) * 128] = jnp.where(seen[c], jnp.exp(exponent), 0.0)
        tail = tail + jnp.sum(keeps[c], axis=1, keepdims=True)
    loads[4].wait()
    for i in range(tokens):
        head_rows[i * heads : (i + 1) * heads, :] = jnp.dot(
            weight_rows[i * heads : (i + 1) * heads, :].astype(bf16),
            values[i],
            preferred_element_type=f32,
        )
    h_out[...] = head_rows[:rows, :].astype(bf16)
    for k in range(1, n_ep):
        to = lax.rem(ep + k, n_ep)
        push(h_out, h_in.at[ep], (to, tp), h_send.at[k], h_recv.at[ep])
    pltpu.make_async_copy(h_out, h_in.at[ep], h_recv.at[ep]).start()

    loads[5].wait()
    for e in range(n_ep):
        arrived(h_in.at[e], h_recv.at[e])
        head_rows[e * rows : (e + 1) * rows, :] = h_in[e].astype(f32)
    summed = x_all[...] * (1.0 / n_tp)
    for h in range(heads):
        summed = summed + jnp.dot(
            head_rows[pl.ds(h, total, stride=heads), :].astype(bf16),
            out_w[h * head_size : (h + 1) * head_size, :],
            preferred_element_type=f32,
        )
    picked = jnp.dot(pick, summed.astype(bf16), preferred_element_type=f32)
    for e in range(n_ep):
        a_out[e] = picked[e * n_ep : (e + 1) * n_ep, :].astype(bf16)
    for i, j in others:
        to, side = lax.rem(ep + i, n_ep), lax.rem(tp + j, n_tp)
        index = i * n_tp + j
        push(a_out.at[to], a_in.at[ep, tp], (to, side), a_send.at[index], a_recv.at[ep, tp])
    pltpu.make_async_copy(a_out.at[ep], a_in.at[ep, tp], a_recv.at[ep, tp]).start()

    for e in range(n_ep):
        m_out[e] = summed[e * tokens : (e + 1) * tokens, :].astype(bf16)
    side, place = ep // per_part, lax.rem(ep, per_part)
    for k in range(1, n_ep):
        to = lax.rem(ep + k, n_ep)
        push(m_out.at[to], m_in.at[place, tp], (to, side), m_send.at[k], m_recv.at[place, tp])

    own = pltpu.make_async_remote_copy(
        src_ref=m_out.at[ep],
        dst_ref=m_in.at[place, tp],
        send_sem=m_send.at[0],
        recv_sem=m_recv.at[place, tp],
        device_id=(ep, side),
        device_id_type=MESH,
    )

    @pl.when(side != tp)
    def _():
        own.start()

    @pl.when(side == tp)
    def _():
        pltpu.make_async_copy(m_out.at[ep], m_in.at[place, tp], m_recv.at[place, tp]).start()

    for load in loads[6:]:
        load.wait()
    gated = jnp.zeros((n_ep, gate_w.shape[1]), f32)
    upped = jnp.zeros((n_ep, up_w.shape[1]), f32)
    squares = jnp.zeros((n_ep, 1), f32)
    for e in range(n_ep):
        for t in range(n_tp):
            arrived(a_in.at[e, t], a_recv.at[e, t])
        block = a_in[e, 0].astype(f32)
        for t in range(1, n_tp):
            block = block + a_in[e, t].astype(f32)
        block = block.astype(bf16).astype(f32)
        squares = squares + jnp.sum(block * block, axis=1, keepdims=True)
        block = (block * moe_gain[:, e * chunk : (e + 1) * chunk]).astype(bf16)
        gated = gated + jnp.dot(
            block, gate_w[e * chunk : (e + 1) * chunk, :], preferred_element_type=f32
        )
        upped = upped + jnp.dot(
            block, up_w[e * chunk : (e + 1) * chunk, :], preferred_element_type=f32
        )
    scale_two = lax.rsqrt(squares * (1.0 / d_model) + rms_epsilon)
    gated = gated * scale_two
    upped = upped * scale_two
    act = (gated / (1.0 + jnp.exp(-gated)) * upped).astype(bf16)
    for t in range(n_tp):
        down = jnp.dot(act, down_w[:, t * part : (t + 1) * part], preferred_element_type=f32)
        for e in range(n_ep):
            z_out[e, t] = down[e : e + 1, :]
    for i, j in others:
        to, side_to = lax.rem(ep + i, n_ep), lax.rem(tp + j, n_tp)
        index = i * n_tp + j
        push(
            z_out.at[to, side_to],
            z_in.at[ep, tp],
            (to, side_to),
            z_send.at[index],
            z_recv.at[ep, tp],
        )
    pltpu.make_async_copy(z_out.at[ep, tp], z_in.at[ep, tp], z_recv.at[ep, tp]).start()

    pieces = []
    for c in range(per_part):
        for t in range(n_tp):
            arrived(m_in.at[c, t], m_recv.at[c, t])
        piece = m_in[c, 0].astype(f32)
        for t in range(1, n_tp):
            piece = piece + m_in[c, t].astype(f32)
        pieces.append(piece.astype(bf16).astype(f32))
    result = jnp.concatenate(pieces, axis=1)
    token = lax.broadcasted_iota(jnp.int32, (tokens, 128), 0)
    expert = lax.broadcasted_iota(jnp.int32, (tokens, 128), 1)
    mixing = jnp.zeros((tokens, 128), f32)
    for k in range(slots):
        share = route_weight[:, k : k + 1].astype(f32)
        for i in range(tokens):
            mixing = mixing + jnp.where((token == i) & (expert == chosen[i][k]), share, 0.0)
    for e in range(n_ep):
        for t in range(n_tp):
            arrived(z_in.at[e, t], z_recv.at[e, t])
        line = z_in[e, 0]
        for t in range(1, n_tp):
            line = line + z_in[e, t]
        result = result + mixing[:, e : e + 1] * line
    mixed[...] = result.astype(bf16)

    for copy in sends:
        copy.wait_send()

    @pl.when(side != tp)
    def _():
        own.wait_send()


def layer(
    hidden,
    attn_gain,
    query_weight,
    head_bias,
    key_cache,
    value_cache,
    lengths,
    out_weight,
    moe_gain,
    route_group,
    route_inner,
    route_weight,
    gate_w,
    up_w,
    down_w,
):
    n_tp = lax.axis_size("tp")
    n_ep = lax.axis_size("ep")
    tokens, d_model = hidden.shape
    _, local_kv, cache_len, head_size = key_cache.shape
    chunk, width = query_weight.shape
    part = d_model // n_tp
    heads = width // head_size
    rows = tokens * heads
    slots = route_inner.shape[1]
    experts = gate_w.shape[0] * n_ep
    fits = (
        gate_w.shape[0] == 1
        and local_kv == 1
        and chunk % 128 == 0
        and part % chunk == 0
        and n_ep % 8 == 0
        and n_ep <= 16
        and rows % 16 == 0
        and head_size == 128
        and cache_len % 128 == 0
        and tokens * n_ep <= 128
    )
    if not fits:
        return body(
            hidden,
            attn_gain,
            query_weight,
            head_bias,
            key_cache,
            value_cache,
            lengths,
            out_weight,
            moe_gain,
            route_group,
            route_inner,
            route_weight,
            gate_w,
            up_w,
            down_w,
        )
    group_size = experts // max(2, experts // 32)
    f32, bf16 = jnp.float32, jnp.bfloat16
    smem = pl.BlockSpec(memory_space=pltpu.SMEM)
    hbm = pl.BlockSpec(memory_space=pl.ANY)
    vmem = pltpu.VMEM
    dma = pltpu.SemaphoreType.DMA
    everyone = n_ep * n_tp
    return pl.pallas_call(
        functools.partial(kernel, n_ep, n_tp, group_size),
        out_shape=jax.ShapeDtypeStruct((tokens, part), bf16),
        in_specs=[smem] * 4 + [hbm] * 11,
        out_specs=pl.BlockSpec(memory_space=pltpu.VMEM),
        scratch_shapes=[
            vmem(hidden.shape, bf16),
            vmem((1, d_model), f32),
            vmem(query_weight.shape, bf16),
            vmem((tokens, cache_len, head_size), bf16),
            vmem((tokens, cache_len, head_size), bf16),
            vmem(out_weight.shape, bf16),
            vmem((1, d_model), f32),
            vmem(route_weight.shape, bf16),
            vmem(gate_w.shape[1:], bf16),
            vmem(up_w.shape[1:], bf16),
            vmem(down_w.shape[1:], bf16),
            dma((11,)),
            vmem((n_ep, tokens, chunk), bf16),
            vmem((1, slots * 128), jnp.int32),
            vmem((n_ep, 1, slots * 128), jnp.int32),
            vmem((n_ep, tokens, width), f32),
            vmem((n_ep, tokens, width), f32),
            vmem((rows, head_size), bf16),
            vmem((n_ep, rows, head_size), bf16),
            vmem((n_ep, n_ep, chunk), bf16),
            vmem((n_ep, n_tp, n_ep, chunk), bf16),
            vmem((n_ep, tokens, chunk), bf16),
            vmem((part // chunk, n_tp, tokens, chunk), bf16),
            vmem((n_ep, n_tp, 1, part), f32),
            vmem((n_ep, n_tp, 1, part), f32),
            dma((n_ep,)),
            dma((n_ep,)),
            dma((n_ep,)),
            dma((n_ep,)),
            dma((n_ep,)),
            dma((n_ep,)),
            dma((n_ep,)),
            dma((n_ep,)),
            dma((everyone,)),
            dma((n_ep, n_tp)),
            dma((n_ep,)),
            dma((part // chunk, n_tp)),
            dma((everyone,)),
            dma((n_ep, n_tp)),
            vmem((tokens * n_ep, chunk), f32),
            vmem((slots, n_ep, 128), jnp.int32),
            vmem((rows, head_size), f32),
            vmem((rows, cache_len), f32),
            vmem((rows, cache_len), f32),
            vmem((rows * n_ep, head_size), f32),
        ],
        compiler_params=pltpu.CompilerParams(
            collective_id=0, has_side_effects=True, vmem_limit_bytes=60 * 1024 * 1024
        ),
    )(
        head_bias,
        lengths,
        route_group,
        route_inner,
        hidden,
        attn_gain.reshape(1, d_model),
        query_weight,
        key_cache,
        value_cache,
        out_weight,
        moe_gain.reshape(1, d_model),
        route_weight,
        gate_w,
        up_w,
        down_w,
    )


def solution(mesh):
    placed = (
        P("ep", None),
        P(),
        P("ep", "tp"),
        P(),
        P("ep", "tp", None, None),
        P("ep", "tp", None, None),
        P("ep"),
        P("tp", "ep"),
        P(),
        P("ep"),
        P("ep", None),
        P("ep", None),
        P("ep", None, "tp"),
        P("ep", None, "tp"),
        P("ep", "tp", None),
    )
    return jax.shard_map(layer, mesh=mesh, in_specs=placed, out_specs=P("ep", "tp"), check_vma=False)
```

```python
import functools

import jax
import jax.numpy as jnp
from jax import lax
from jax.experimental import pallas as pl
from jax.experimental.pallas import tpu as pltpu
from jax.sharding import PartitionSpec as P

rms_epsilon = 1e-06


def rms_scale(values, gain):
    wide = values.astype(jnp.float32)
    scaled = wide * lax.rsqrt(jnp.mean(wide * wide, axis=-1, keepdims=True) + rms_epsilon)
    return (scaled * gain).astype(jnp.bfloat16)


def body(
    hidden,
    attn_gain,
    query_weight,
    head_bias,
    key_cache,
    value_cache,
    lengths,
    out_weight,
    moe_gain,
    route_group,
    route_inner,
    route_weight,
    gate_w,
    up_w,
    down_w,
):
    n_tp = lax.axis_size("tp")
    n_ep = lax.axis_size("ep")
    tokens = hidden.shape[0]
    d_model = hidden.shape[1]
    normed = rms_scale(hidden, attn_gain)
    feature_block = lax.all_to_all(normed, "ep", split_axis=1, concat_axis=0, tiled=True)
    queries = lax.psum_scatter(
        jnp.dot(feature_block, query_weight, preferred_element_type=jnp.float32),
        "ep",
        scatter_dimension=0,
        tiled=True,
    ).astype(jnp.bfloat16)
    head_size = key_cache.shape[3]
    local_kv = key_cache.shape[1]
    cache_len = key_cache.shape[2]
    local_heads = queries.shape[1] // head_size
    group_heads = local_heads // local_kv
    queries = queries.reshape(tokens, local_kv, group_heads, head_size)
    own_bias = lax.dynamic_slice_in_dim(
        head_bias, lax.axis_index("tp") * local_heads, local_heads, 0
    )
    own_bias = own_bias.reshape(local_kv, group_heads)
    scores = jnp.einsum(
        "tkgd,tkpd->tkgp", queries, key_cache, preferred_element_type=jnp.float32
    ) * head_size ** (-0.5)
    scores = scores + own_bias[None, :, :, None]
    position = jnp.arange(cache_len, dtype=jnp.int32)
    visible = position[None, None, None, :] < lengths[:, None, None, None]
    log_keep = jnp.where(visible, jax.nn.log_sigmoid(-scores), 0.0)
    later_sum = lax.cumsum(log_keep, axis=3, reverse=True) - log_keep
    weight = jnp.where(visible, jnp.exp(jax.nn.log_sigmoid(scores) + later_sum), 0.0).astype(
        jnp.bfloat16
    )
    heads_out = jnp.einsum(
        "tkgp,tkpd->tkgd", weight, value_cache, preferred_element_type=jnp.float32
    )
    heads_out = heads_out.astype(jnp.bfloat16).reshape(tokens, -1)
    partial_value = jnp.dot(
        heads_out,
        lax.all_gather(out_weight, "ep", axis=1, tiled=True),
        preferred_element_type=jnp.float32,
    )
    rounded = lax.optimization_barrier(partial_value.astype(jnp.bfloat16)).astype(jnp.float32)
    attended = lax.psum(rounded.astype(jnp.bfloat16), "tp").astype(jnp.float32)
    residual = (hidden.astype(jnp.float32) + attended).astype(jnp.bfloat16)
    normed_two = rms_scale(residual, moe_gain)
    per_device = gate_w.shape[0]
    experts = per_device * n_ep
    group_count = max(2, experts // 32)
    group_size = experts // group_count
    chosen = route_group[:, None] * group_size + route_inner
    matches = chosen[:, :, None] == jnp.arange(experts, dtype=jnp.int32)[None, None, :]
    picked = jnp.any(matches, axis=1).astype(jnp.bfloat16)
    mixing = jnp.sum(
        jnp.where(matches, route_weight[:, :, None].astype(jnp.float32), 0.0), axis=1
    ).astype(jnp.bfloat16)
    part_width = d_model // n_tp
    outgoing = jnp.einsum("te,td->ed", picked, normed_two, preferred_element_type=jnp.float32)
    outgoing = outgoing.astype(jnp.bfloat16).reshape(n_ep, per_device, d_model)
    arrived = lax.all_to_all(outgoing, "ep", split_axis=0, concat_axis=0, tiled=True)
    gated_in = jnp.einsum("sed,edf->sef", arrived, gate_w, preferred_element_type=jnp.float32)
    up_proj = jnp.einsum("sed,edf->sef", arrived, up_w, preferred_element_type=jnp.float32)
    activated = (jax.nn.silu(gated_in) * up_proj).astype(jnp.bfloat16)
    down_out = jnp.einsum("sef,efd->sed", activated, down_w, preferred_element_type=jnp.float32)
    down_rounded = lax.optimization_barrier(down_out.astype(jnp.bfloat16)).astype(jnp.float32)
    summed = lax.psum_scatter(
        down_rounded.astype(jnp.bfloat16), "tp", scatter_dimension=2, tiled=True
    )
    returned = lax.all_to_all(summed, "ep", split_axis=0, concat_axis=0, tiled=True).reshape(
        experts, part_width
    )
    routed = jnp.dot(mixing, returned, preferred_element_type=jnp.float32)
    own_residual = lax.dynamic_slice_in_dim(
        residual, lax.axis_index("tp") * part_width, part_width, 1
    )
    return (own_residual.astype(jnp.float32) + routed).astype(jnp.bfloat16)


MESH = pl.DeviceIdType.MESH


def kernel(
    n_ep,
    n_tp,
    group_size,
    head_bias,
    lengths,
    route_group,
    route_inner,
    hidden_hbm,
    attn_gain_hbm,
    query_hbm,
    key_hbm,
    value_hbm,
    out_hbm,
    moe_gain_hbm,
    route_weight_hbm,
    gate_hbm,
    up_hbm,
    down_hbm,
    mixed,
    hidden,
    attn_gain,
    query_w,
    keys,
    values,
    out_w,
    moe_gain,
    route_weight,
    gate_w,
    up_w,
    down_w,
    load_sem,
    x_in,
    r_out,
    r_in,
    q_out,
    q_in,
    h_out,
    h_in,
    a_out,
    a_in,
    m_out,
    m_in,
    z_out,
    z_in,
    x_send,
    x_recv,
    r_send,
    r_recv,
    q_send,
    q_recv,
    h_send,
    h_recv,
    a_send,
    a_recv,
    m_send,
    m_recv,
    z_send,
    z_recv,
    x_all,
    route_all,
    q_rows,
    score_rows,
    weight_rows,
    head_rows,
):
    f32, bf16 = jnp.float32, jnp.bfloat16
    ep = lax.axis_index("ep")
    tp = lax.axis_index("tp")
    tokens, d_model = hidden.shape
    chunk = d_model // n_ep
    total = tokens * n_ep
    cache_len, head_size = keys.shape[1], keys.shape[2]
    heads = query_w.shape[1] // head_size
    rows = tokens * heads
    part = d_model // n_tp
    per_part = part // chunk
    slots = route_inner.shape[0]

    loads = [
        pltpu.make_async_copy(src, dst, load_sem.at[index])
        for index, (src, dst) in enumerate(
            (
                (hidden_hbm, hidden),
                (attn_gain_hbm, attn_gain),
                (query_hbm, query_w),
                (key_hbm.at[:, 0], keys),
                (value_hbm.at[:, 0], values),
                (out_hbm, out_w),
                (moe_gain_hbm, moe_gain),
                (route_weight_hbm, route_weight),
                (gate_hbm.at[0], gate_w),
                (up_hbm.at[0], up_w),
                (down_hbm.at[0], down_w),
            )
        )
    ]
    for load in loads:
        load.start()

    barrier = pltpu.get_barrier_semaphore()
    others = [(i, j) for i in range(n_ep) for j in range(n_tp) if (i, j) != (0, 0)]
    for i, j in others:
        peer = (lax.rem(ep + i, n_ep), lax.rem(tp + j, n_tp))
        pl.semaphore_signal(barrier, inc=1, device_id=peer, device_id_type=MESH)

    lane = lax.broadcasted_iota(jnp.int32, (1, slots * 128), 1)
    own_route = jnp.full((1, slots * 128), -1, jnp.int32)
    chosen = [
        [route_group[i] * group_size + route_inner[k, i] for k in range(slots)]
        for i in range(tokens)
    ]
    for i in range(tokens):
        for k in range(slots):
            own_route = jnp.where(lane == k * 128 + ep * tokens + i, chosen[i][k], own_route)
    r_out[...] = own_route

    pl.semaphore_wait(barrier, len(others))
    loads[0].wait()

    sends = []

    def push(src, dst, peer, send_sem, recv_sem):
        copy = pltpu.make_async_remote_copy(
            src_ref=src,
            dst_ref=dst,
            send_sem=send_sem,
            recv_sem=recv_sem,
            device_id=peer,
            device_id_type=MESH,
        )
        copy.start()
        sends.append(copy)

    def arrived(ref, sem):
        pltpu.make_async_copy(ref, ref, sem).wait()

    def columns(index, width):
        return pl.ds(pl.multiple_of(index * width, 128), width)

    for k in range(1, n_ep):
        to = lax.rem(ep + k, n_ep)
        push(hidden.at[:, columns(to, chunk)], x_in.at[ep], (to, tp), x_send.at[k], x_recv.at[ep])
    pltpu.make_async_copy(hidden.at[:, columns(ep, chunk)], x_in.at[ep], x_recv.at[ep]).start()
    for k in range(1, n_ep):
        to = lax.rem(ep + k, n_ep)
        push(r_out, r_in.at[ep], (to, tp), r_send.at[k], r_recv.at[ep])
    pltpu.make_async_copy(r_out, r_in.at[ep], r_recv.at[ep]).start()

    wide = hidden[...].astype(f32)
    scale = lax.rsqrt(jnp.mean(wide * wide, axis=-1, keepdims=True) + rms_epsilon)

    loads[7].wait()
    shares = route_weight[...].astype(f32)
    token = lax.broadcasted_iota(jnp.int32, (tokens, 128), 0)
    expert = lax.broadcasted_iota(jnp.int32, (tokens, 128), 1)
    mixing = jnp.zeros((tokens, 128), f32)
    for k in range(slots):
        for i in range(tokens):
            mixing = mixing + jnp.where(
                (token == i) & (expert == chosen[i][k]), shares[k : k + 1, i : i + 1], 0.0
            )

    loads[1].wait()
    loads[2].wait()
    for e in range(n_ep):
        arrived(x_in.at[e], x_recv.at[e])
        x_all[e * tokens : (e + 1) * tokens, :] = x_in[e].astype(f32)
    features = (x_all[...] * attn_gain[:, columns(ep, chunk)]).astype(bf16)
    query_parts = jnp.dot(features, query_w[...], preferred_element_type=f32)
    for e in range(n_ep):
        q_out[e] = query_parts[e * tokens : (e + 1) * tokens, :]
    for k in range(1, n_ep):
        to = lax.rem(ep + k, n_ep)
        push(q_out.at[to], q_in.at[ep], (to, tp), q_send.at[k], q_recv.at[ep])
    pltpu.make_async_copy(q_out.at[ep], q_in.at[ep], q_recv.at[ep]).start()

    for e in range(n_ep):
        arrived(r_in.at[e], r_recv.at[e])
        for k in range(slots):
            route_all[k, e : e + 1, :] = r_in[e, :, k * 128 : (k + 1) * 128]
    tables = [route_all[k] for k in range(slots)]
    picks = []
    for e in range(n_ep):
        hit = tables[0] == e
        for table in tables[1:]:
            hit = hit | (table == e)
        picks.append(jnp.where(hit, 1.0, 0.0))
    pick = jnp.concatenate(picks, axis=0)[:, :total].astype(bf16)

    row = lax.broadcasted_iota(jnp.int32, (rows, 1), 0)
    bias = jnp.zeros((rows, 1), f32)
    length = jnp.zeros((rows, 1), jnp.int32)
    for i in range(tokens):
        length = jnp.where(row // heads == i, lengths[i], length)
    for h in range(heads):
        bias = jnp.where(row % heads == h, head_bias[tp * heads + h], bias)
    above = lax.broadcasted_iota(jnp.int32, (128, 128), 0) > lax.broadcasted_iota(
        jnp.int32, (128, 128), 1
    )
    above = jnp.where(above, 1.0, 0.0).astype(bf16)
    loads[3].wait()

    for e in range(n_ep):
        arrived(q_in.at[e], q_recv.at[e])
    queries = q_in[0]
    for e in range(1, n_ep):
        queries = queries + q_in[e]
    queries = queries * scale
    for i in range(tokens):
        for h in range(heads):
            q_rows[i * heads + h : i * heads + h + 1, :] = queries[
                i : i + 1, h * head_size : (h + 1) * head_size
            ]
    for i in range(tokens):
        score_rows[i * heads : (i + 1) * heads, :] = lax.dot_general(
            q_rows[i * heads : (i + 1) * heads, :].astype(bf16),
            keys[i],
            (((1,), (1,)), ((), ())),
            preferred_element_type=f32,
        )
    blocks = cache_len // 128
    keeps, takes, seen = [], [], []
    position = lax.broadcasted_iota(jnp.int32, (rows, 128), 1)
    for c in range(blocks):
        score = score_rows[:, c * 128 : (c + 1) * 128] * head_size ** (-0.5) + bias
        visible = position + c * 128 < length
        soft = jnp.log1p(jnp.exp(-jnp.abs(score)))
        keeps.append(jnp.where(visible, -jnp.maximum(score, 0.0) - soft, 0.0))
        takes.append(jnp.minimum(score, 0.0) - soft)
        seen.append(visible)
    keep = jnp.concatenate(keeps, axis=0)
    high = keep.astype(bf16)
    rest = keep - high.astype(f32)
    middle = rest.astype(bf16)
    low = (rest - middle.astype(f32)).astype(bf16)
    later = (
        jnp.dot(high, above, preferred_element_type=f32)
        + jnp.dot(middle, above, preferred_element_type=f32)
        + jnp.dot(low, above, preferred_element_type=f32)
    )
    tail = jnp.zeros((rows, 1), f32)
    for c in reversed(range(blocks)):
        exponent = takes[c] + later[c * rows : (c + 1) * rows, :] + tail
        weight_rows[:, c * 128 : (c + 1) * 128] = jnp.where(seen[c], jnp.exp(exponent), 0.0)
        tail = tail + jnp.sum(keeps[c], axis=1, keepdims=True)
    loads[4].wait()
    for i in range(tokens):
        head_rows[i * heads : (i + 1) * heads, :] = jnp.dot(
            weight_rows[i * heads : (i + 1) * heads, :].astype(bf16),
            values[i],
            preferred_element_type=f32,
        )
    h_out[...] = head_rows[:rows, :].astype(bf16)
    for k in range(1, n_ep):
        to = lax.rem(ep + k, n_ep)
        push(h_out, h_in.at[ep], (to, tp), h_send.at[k], h_recv.at[ep])
    pltpu.make_async_copy(h_out, h_in.at[ep], h_recv.at[ep]).start()

    loads[5].wait()
    for e in range(n_ep):
        arrived(h_in.at[e], h_recv.at[e])
        head_rows[e * rows : (e + 1) * rows, :] = h_in[e].astype(f32)
    summed = x_all[...] * (1.0 / n_tp)
    for h in range(heads):
        summed = summed + jnp.dot(
            head_rows[pl.ds(h, total, stride=heads), :].astype(bf16),
            out_w[h * head_size : (h + 1) * head_size, :],
            preferred_element_type=f32,
        )
    picked = jnp.dot(pick, summed.astype(bf16), preferred_element_type=f32)
    for e in range(n_ep):
        a_out[e] = picked[e * n_ep : (e + 1) * n_ep, :].astype(bf16)
    for i, j in others:
        to, side = lax.rem(ep + i, n_ep), lax.rem(tp + j, n_tp)
        index = i * n_tp + j
        push(a_out.at[to], a_in.at[ep, tp], (to, side), a_send.at[index], a_recv.at[ep, tp])
    pltpu.make_async_copy(a_out.at[ep], a_in.at[ep, tp], a_recv.at[ep, tp]).start()

    for e in range(n_ep):
        m_out[e] = summed[e * tokens : (e + 1) * tokens, :].astype(bf16)
    side, place = ep // per_part, lax.rem(ep, per_part)
    for k in range(1, n_ep):
        to = lax.rem(ep + k, n_ep)
        push(m_out.at[to], m_in.at[place, tp], (to, side), m_send.at[k], m_recv.at[place, tp])

    own = pltpu.make_async_remote_copy(
        src_ref=m_out.at[ep],
        dst_ref=m_in.at[place, tp],
        send_sem=m_send.at[0],
        recv_sem=m_recv.at[place, tp],
        device_id=(ep, side),
        device_id_type=MESH,
    )

    @pl.when(side != tp)
    def _():
        own.start()

    @pl.when(side == tp)
    def _():
        pltpu.make_async_copy(m_out.at[ep], m_in.at[place, tp], m_recv.at[place, tp]).start()

    for load in (loads[6], loads[8], loads[9], loads[10]):
        load.wait()
    gated = jnp.zeros((n_ep, gate_w.shape[0]), f32)
    upped = jnp.zeros((n_ep, up_w.shape[0]), f32)
    squares = jnp.zeros((n_ep, 1), f32)
    for e in range(n_ep):
        for t in range(n_tp):
            arrived(a_in.at[e, t], a_recv.at[e, t])
        block = a_in[e, 0].astype(f32)
        for t in range(1, n_tp):
            block = block + a_in[e, t].astype(f32)
        block = block.astype(bf16).astype(f32)
        squares = squares + jnp.sum(block * block, axis=1, keepdims=True)
        block = (block * moe_gain[:, e * chunk : (e + 1) * chunk]).astype(bf16)
        gated = gated + lax.dot_general(
            block,
            gate_w[:, e * chunk : (e + 1) * chunk],
            (((1,), (1,)), ((), ())),
            preferred_element_type=f32,
        )
        upped = upped + lax.dot_general(
            block,
            up_w[:, e * chunk : (e + 1) * chunk],
            (((1,), (1,)), ((), ())),
            preferred_element_type=f32,
        )
    scale_two = lax.rsqrt(squares * (1.0 / d_model) + rms_epsilon)
    gated = gated * scale_two
    upped = upped * scale_two
    act = (gated / (1.0 + jnp.exp(-gated)) * upped).astype(bf16)
    for t in range(n_tp):
        down = jnp.dot(act, down_w[:, t * part : (t + 1) * part], preferred_element_type=f32)
        for e in range(n_ep):
            z_out[e, t] = down[e : e + 1, :]
    for i, j in others:
        to, side_to = lax.rem(ep + i, n_ep), lax.rem(tp + j, n_tp)
        index = i * n_tp + j
        push(
            z_out.at[to, side_to],
            z_in.at[ep, tp],
            (to, side_to),
            z_send.at[index],
            z_recv.at[ep, tp],
        )
    pltpu.make_async_copy(z_out.at[ep, tp], z_in.at[ep, tp], z_recv.at[ep, tp]).start()

    pieces = []
    for c in range(per_part):
        for t in range(n_tp):
            arrived(m_in.at[c, t], m_recv.at[c, t])
        piece = m_in[c, 0].astype(f32)
        for t in range(1, n_tp):
            piece = piece + m_in[c, t].astype(f32)
        pieces.append(piece.astype(bf16).astype(f32))
    result = jnp.concatenate(pieces, axis=1)
    for e in range(n_ep):
        for t in range(n_tp):
            arrived(z_in.at[e, t], z_recv.at[e, t])
        line = z_in[e, 0]
        for t in range(1, n_tp):
            line = line + z_in[e, t]
        result = result + mixing[:, e : e + 1] * line
    mixed[...] = result.astype(bf16)

    for copy in sends:
        copy.wait_send()

    @pl.when(side != tp)
    def _():
        own.wait_send()


def layer(
    hidden,
    attn_gain,
    query_weight,
    head_bias,
    key_cache,
    value_cache,
    lengths,
    out_weight,
    moe_gain,
    route_group,
    route_inner,
    route_weight,
    gate_w,
    up_w,
    down_w,
):
    n_tp = lax.axis_size("tp")
    n_ep = lax.axis_size("ep")
    tokens, d_model = hidden.shape
    _, local_kv, cache_len, head_size = key_cache.shape
    chunk, width = query_weight.shape
    part = d_model // n_tp
    heads = width // head_size
    rows = tokens * heads
    slots = route_inner.shape[1]
    experts = gate_w.shape[0] * n_ep
    fits = (
        gate_w.shape[0] == 1
        and local_kv == 1
        and chunk % 128 == 0
        and part % chunk == 0
        and n_ep % 8 == 0
        and n_ep <= 16
        and rows % 16 == 0
        and head_size == 128
        and cache_len % 128 == 0
        and tokens * n_ep <= 128
    )
    if not fits:
        return body(
            hidden,
            attn_gain,
            query_weight,
            head_bias,
            key_cache,
            value_cache,
            lengths,
            out_weight,
            moe_gain,
            route_group,
            route_inner,
            route_weight,
            gate_w,
            up_w,
            down_w,
        )
    group_size = experts // max(2, experts // 32)
    f32, bf16 = jnp.float32, jnp.bfloat16
    smem = pl.BlockSpec(memory_space=pltpu.SMEM)
    hbm = pl.BlockSpec(memory_space=pl.ANY)
    vmem = pltpu.VMEM
    dma = pltpu.SemaphoreType.DMA
    everyone = n_ep * n_tp
    return pl.pallas_call(
        functools.partial(kernel, n_ep, n_tp, group_size),
        out_shape=jax.ShapeDtypeStruct((tokens, part), bf16),
        in_specs=[smem] * 4 + [hbm] * 11,
        out_specs=pl.BlockSpec(memory_space=pltpu.VMEM),
        scratch_shapes=[
            vmem(hidden.shape, bf16),
            vmem((1, d_model), f32),
            vmem(query_weight.shape, bf16),
            vmem((tokens, cache_len, head_size), bf16),
            vmem((tokens, cache_len, head_size), bf16),
            vmem(out_weight.shape, bf16),
            vmem((1, d_model), f32),
            vmem((slots, tokens), bf16),
            vmem((gate_w.shape[2], d_model), bf16),
            vmem((up_w.shape[2], d_model), bf16),
            vmem(down_w.shape[1:], bf16),
            dma((11,)),
            vmem((n_ep, tokens, chunk), bf16),
            vmem((1, slots * 128), jnp.int32),
            vmem((n_ep, 1, slots * 128), jnp.int32),
            vmem((n_ep, tokens, width), f32),
            vmem((n_ep, tokens, width), f32),
            vmem((rows, head_size), bf16),
            vmem((n_ep, rows, head_size), bf16),
            vmem((n_ep, n_ep, chunk), bf16),
            vmem((n_ep, n_tp, n_ep, chunk), bf16),
            vmem((n_ep, tokens, chunk), bf16),
            vmem((part // chunk, n_tp, tokens, chunk), bf16),
            vmem((n_ep, n_tp, 1, part), f32),
            vmem((n_ep, n_tp, 1, part), f32),
            dma((n_ep,)),
            dma((n_ep,)),
            dma((n_ep,)),
            dma((n_ep,)),
            dma((n_ep,)),
            dma((n_ep,)),
            dma((n_ep,)),
            dma((n_ep,)),
            dma((everyone,)),
            dma((n_ep, n_tp)),
            dma((n_ep,)),
            dma((part // chunk, n_tp)),
            dma((everyone,)),
            dma((n_ep, n_tp)),
            vmem((tokens * n_ep, chunk), f32),
            vmem((slots, n_ep, 128), jnp.int32),
            vmem((rows, head_size), f32),
            vmem((rows, cache_len), f32),
            vmem((rows, cache_len), f32),
            vmem((rows * n_ep, head_size), f32),
        ],
        compiler_params=pltpu.CompilerParams(
            collective_id=0, has_side_effects=True, vmem_limit_bytes=60 * 1024 * 1024
        ),
    )(
        head_bias,
        lengths,
        route_group,
        route_inner.T,
        hidden,
        attn_gain.reshape(1, d_model),
        query_weight,
        key_cache,
        value_cache,
        out_weight,
        moe_gain.reshape(1, d_model),
        route_weight.T,
        gate_w.swapaxes(1, 2),
        up_w.swapaxes(1, 2),
        down_w,
    )


def solution(mesh):
    placed = (
        P("ep", None),
        P(),
        P("ep", "tp"),
        P(),
        P("ep", "tp", None, None),
        P("ep", "tp", None, None),
        P("ep"),
        P("tp", "ep"),
        P(),
        P("ep"),
        P("ep", None),
        P("ep", None),
        P("ep", None, "tp"),
        P("ep", None, "tp"),
        P("ep", "tp", None),
    )
    return jax.shard_map(layer, mesh=mesh, in_specs=placed, out_specs=P("ep", "tp"), check_vma=False)
```

```python
import functools

import jax
import jax.numpy as jnp
from jax import lax
from jax.experimental import pallas as pl
from jax.experimental.pallas import tpu as pltpu
from jax.sharding import PartitionSpec as P

rms_epsilon = 1e-06


def rms_scale(values, gain):
    wide = values.astype(jnp.float32)
    scaled = wide * lax.rsqrt(jnp.mean(wide * wide, axis=-1, keepdims=True) + rms_epsilon)
    return (scaled * gain).astype(jnp.bfloat16)


def body(
    hidden,
    attn_gain,
    query_weight,
    head_bias,
    key_cache,
    value_cache,
    lengths,
    out_weight,
    moe_gain,
    route_group,
    route_inner,
    route_weight,
    gate_w,
    up_w,
    down_w,
):
    n_tp = lax.axis_size("tp")
    n_ep = lax.axis_size("ep")
    tokens = hidden.shape[0]
    d_model = hidden.shape[1]
    normed = rms_scale(hidden, attn_gain)
    feature_block = lax.all_to_all(normed, "ep", split_axis=1, concat_axis=0, tiled=True)
    queries = lax.psum_scatter(
        jnp.dot(feature_block, query_weight, preferred_element_type=jnp.float32),
        "ep",
        scatter_dimension=0,
        tiled=True,
    ).astype(jnp.bfloat16)
    head_size = key_cache.shape[3]
    local_kv = key_cache.shape[1]
    cache_len = key_cache.shape[2]
    local_heads = queries.shape[1] // head_size
    group_heads = local_heads // local_kv
    queries = queries.reshape(tokens, local_kv, group_heads, head_size)
    own_bias = lax.dynamic_slice_in_dim(
        head_bias, lax.axis_index("tp") * local_heads, local_heads, 0
    )
    own_bias = own_bias.reshape(local_kv, group_heads)
    scores = jnp.einsum(
        "tkgd,tkpd->tkgp", queries, key_cache, preferred_element_type=jnp.float32
    ) * head_size ** (-0.5)
    scores = scores + own_bias[None, :, :, None]
    position = jnp.arange(cache_len, dtype=jnp.int32)
    visible = position[None, None, None, :] < lengths[:, None, None, None]
    log_keep = jnp.where(visible, jax.nn.log_sigmoid(-scores), 0.0)
    later_sum = lax.cumsum(log_keep, axis=3, reverse=True) - log_keep
    weight = jnp.where(visible, jnp.exp(jax.nn.log_sigmoid(scores) + later_sum), 0.0).astype(
        jnp.bfloat16
    )
    heads_out = jnp.einsum(
        "tkgp,tkpd->tkgd", weight, value_cache, preferred_element_type=jnp.float32
    )
    heads_out = heads_out.astype(jnp.bfloat16).reshape(tokens, -1)
    partial_value = jnp.dot(
        heads_out,
        lax.all_gather(out_weight, "ep", axis=1, tiled=True),
        preferred_element_type=jnp.float32,
    )
    rounded = lax.optimization_barrier(partial_value.astype(jnp.bfloat16)).astype(jnp.float32)
    attended = lax.psum(rounded.astype(jnp.bfloat16), "tp").astype(jnp.float32)
    residual = (hidden.astype(jnp.float32) + attended).astype(jnp.bfloat16)
    normed_two = rms_scale(residual, moe_gain)
    per_device = gate_w.shape[0]
    experts = per_device * n_ep
    group_count = max(2, experts // 32)
    group_size = experts // group_count
    chosen = route_group[:, None] * group_size + route_inner
    matches = chosen[:, :, None] == jnp.arange(experts, dtype=jnp.int32)[None, None, :]
    picked = jnp.any(matches, axis=1).astype(jnp.bfloat16)
    mixing = jnp.sum(
        jnp.where(matches, route_weight[:, :, None].astype(jnp.float32), 0.0), axis=1
    ).astype(jnp.bfloat16)
    part_width = d_model // n_tp
    outgoing = jnp.einsum("te,td->ed", picked, normed_two, preferred_element_type=jnp.float32)
    outgoing = outgoing.astype(jnp.bfloat16).reshape(n_ep, per_device, d_model)
    arrived = lax.all_to_all(outgoing, "ep", split_axis=0, concat_axis=0, tiled=True)
    gated_in = jnp.einsum("sed,edf->sef", arrived, gate_w, preferred_element_type=jnp.float32)
    up_proj = jnp.einsum("sed,edf->sef", arrived, up_w, preferred_element_type=jnp.float32)
    activated = (jax.nn.silu(gated_in) * up_proj).astype(jnp.bfloat16)
    down_out = jnp.einsum("sef,efd->sed", activated, down_w, preferred_element_type=jnp.float32)
    down_rounded = lax.optimization_barrier(down_out.astype(jnp.bfloat16)).astype(jnp.float32)
    summed = lax.psum_scatter(
        down_rounded.astype(jnp.bfloat16), "tp", scatter_dimension=2, tiled=True
    )
    returned = lax.all_to_all(summed, "ep", split_axis=0, concat_axis=0, tiled=True).reshape(
        experts, part_width
    )
    routed = jnp.dot(mixing, returned, preferred_element_type=jnp.float32)
    own_residual = lax.dynamic_slice_in_dim(
        residual, lax.axis_index("tp") * part_width, part_width, 1
    )
    return (own_residual.astype(jnp.float32) + routed).astype(jnp.bfloat16)


MESH = pl.DeviceIdType.MESH


def kernel(
    n_ep,
    n_tp,
    group_size,
    head_bias_hbm,
    lengths_hbm,
    route_group_hbm,
    route_inner_hbm,
    hidden_hbm,
    attn_gain_hbm,
    query_hbm,
    key_hbm,
    value_hbm,
    out_hbm,
    moe_gain_hbm,
    route_weight_hbm,
    gate_hbm,
    up_hbm,
    down_hbm,
    mixed,
    head_bias,
    lengths,
    route_group,
    route_inner,
    hidden,
    attn_gain,
    query_w,
    keys,
    values,
    out_w,
    moe_gain,
    route_weight,
    gate_w,
    up_w,
    down_w,
    load_sem,
    x_in,
    r_out,
    r_in,
    q_out,
    q_in,
    h_out,
    h_in,
    a_out,
    a_in,
    m_out,
    m_in,
    z_out,
    z_in,
    x_send,
    x_recv,
    r_send,
    r_recv,
    q_send,
    q_recv,
    h_send,
    h_recv,
    a_send,
    a_recv,
    m_send,
    m_recv,
    z_send,
    z_recv,
    x_all,
    route_all,
    q_rows,
    score_rows,
    weight_rows,
    head_rows,
):
    f32, bf16 = jnp.float32, jnp.bfloat16
    ep = lax.axis_index("ep")
    tp = lax.axis_index("tp")
    tokens, d_model = hidden.shape
    chunk = d_model // n_ep
    total = tokens * n_ep
    cache_len, head_size = keys.shape[1], keys.shape[2]
    heads = query_w.shape[1] // head_size
    rows = tokens * heads
    part = d_model // n_tp
    per_part = part // chunk
    slots = route_inner.shape[0]

    loads = [
        pltpu.make_async_copy(src, dst, load_sem.at[index])
        for index, (src, dst) in enumerate(
            (
                (hidden_hbm, hidden),
                (attn_gain_hbm, attn_gain),
                (query_hbm, query_w),
                (key_hbm.at[:, 0], keys),
                (value_hbm.at[:, 0], values),
                (out_hbm, out_w),
                (moe_gain_hbm, moe_gain),
                (route_weight_hbm, route_weight),
                (gate_hbm.at[0], gate_w),
                (up_hbm.at[0], up_w),
                (down_hbm.at[0], down_w),
                (route_group_hbm, route_group),
                (route_inner_hbm, route_inner),
                (lengths_hbm, lengths),
                (head_bias_hbm, head_bias),
            )
        )
    ]
    loads[0].start()

    barrier = pltpu.get_barrier_semaphore()
    others = [(i, j) for i in range(n_ep) for j in range(n_tp) if (i, j) != (0, 0)]
    for i, j in others:
        peer = (lax.rem(ep + i, n_ep), lax.rem(tp + j, n_tp))
        pl.semaphore_signal(barrier, inc=1, device_id=peer, device_id_type=MESH)

    for load in loads[11:13] + loads[1:11] + loads[13:]:
        load.start()

    loads[11].wait()
    loads[12].wait()
    lane = lax.broadcasted_iota(jnp.int32, (1, slots * 128), 1)
    own_route = jnp.full((1, slots * 128), -1, jnp.int32)
    chosen = [
        [route_group[i] * group_size + route_inner[k, i] for k in range(slots)]
        for i in range(tokens)
    ]
    for i in range(tokens):
        for k in range(slots):
            own_route = jnp.where(lane == k * 128 + ep * tokens + i, chosen[i][k], own_route)
    r_out[...] = own_route

    pl.semaphore_wait(barrier, len(others))
    loads[0].wait()

    sends = []
    last = n_ep - 1
    upper = ep >= n_ep // 2

    def partner(step):
        down_to = last - step - jnp.where(last - step <= ep, 1, 0)
        up_to = step + jnp.where(step >= ep, 1, 0)
        return jnp.where(upper, up_to, down_to)

    partners = [partner(step) for step in range(last)]

    def push(src, dst, peer, send_sem, recv_sem):
        copy = pltpu.make_async_remote_copy(
            src_ref=src,
            dst_ref=dst,
            send_sem=send_sem,
            recv_sem=recv_sem,
            device_id=peer,
            device_id_type=MESH,
        )
        copy.start()
        sends.append(copy)

    def arrived(ref, sem):
        pltpu.make_async_copy(ref, ref, sem).wait()

    def columns(index, width):
        return pl.ds(pl.multiple_of(index * width, 128), width)

    for k, to in enumerate(partners):
        push(hidden.at[:, columns(to, chunk)], x_in.at[ep], (to, tp), x_send.at[k], x_recv.at[ep])
    pltpu.make_async_copy(hidden.at[:, columns(ep, chunk)], x_in.at[ep], x_recv.at[ep]).start()
    for k, to in enumerate(partners):
        push(r_out, r_in.at[ep], (to, tp), r_send.at[k], r_recv.at[ep])
    pltpu.make_async_copy(r_out, r_in.at[ep], r_recv.at[ep]).start()

    wide = hidden[...].astype(f32)
    scale = lax.rsqrt(jnp.mean(wide * wide, axis=-1, keepdims=True) + rms_epsilon)

    loads[7].wait()
    shares = route_weight[...].astype(f32)
    token = lax.broadcasted_iota(jnp.int32, (tokens, 128), 0)
    expert = lax.broadcasted_iota(jnp.int32, (tokens, 128), 1)
    mixing = jnp.zeros((tokens, 128), f32)
    for k in range(slots):
        for i in range(tokens):
            mixing = mixing + jnp.where(
                (token == i) & (expert == chosen[i][k]), shares[k : k + 1, i : i + 1], 0.0
            )

    loads[1].wait()
    loads[2].wait()
    for e in range(n_ep):
        arrived(x_in.at[e], x_recv.at[e])
        x_all[e * tokens : (e + 1) * tokens, :] = x_in[e].astype(f32)
    features = (x_all[...] * attn_gain[:, columns(ep, chunk)]).astype(bf16)
    query_parts = jnp.dot(features, query_w[...], preferred_element_type=f32)
    for e in range(n_ep):
        q_out[e] = query_parts[e * tokens : (e + 1) * tokens, :].astype(bf16)
    for k, to in enumerate(partners):
        push(q_out.at[to], q_in.at[ep], (to, tp), q_send.at[k], q_recv.at[ep])
    pltpu.make_async_copy(q_out.at[ep], q_in.at[ep], q_recv.at[ep]).start()

    for e in range(n_ep):
        arrived(r_in.at[e], r_recv.at[e])
        for k in range(slots):
            route_all[k, e : e + 1, :] = r_in[e, :, k * 128 : (k + 1) * 128]
    tables = [route_all[k] for k in range(slots)]
    picks = []
    for e in range(n_ep):
        hit = tables[0] == e
        for table in tables[1:]:
            hit = hit | (table == e)
        picks.append(jnp.where(hit, 1.0, 0.0))
    pick = jnp.concatenate(picks, axis=0)[:, :total].astype(bf16)

    loads[13].wait()
    loads[14].wait()
    row = lax.broadcasted_iota(jnp.int32, (rows, 1), 0)
    bias = jnp.zeros((rows, 1), f32)
    length = jnp.zeros((rows, 1), jnp.int32)
    for i in range(tokens):
        length = jnp.where(row // heads == i, lengths[i], length)
    for h in range(heads):
        bias = jnp.where(row % heads == h, head_bias[tp * heads + h], bias)
    above = lax.broadcasted_iota(jnp.int32, (128, 128), 0) > lax.broadcasted_iota(
        jnp.int32, (128, 128), 1
    )
    above = jnp.where(above, 1.0, 0.0).astype(bf16)
    loads[3].wait()

    for e in range(n_ep):
        arrived(q_in.at[e], q_recv.at[e])
    queries = q_in[0].astype(f32)
    for e in range(1, n_ep):
        queries = queries + q_in[e].astype(f32)
    queries = queries * scale
    for i in range(tokens):
        for h in range(heads):
            q_rows[i * heads + h : i * heads + h + 1, :] = queries[
                i : i + 1, h * head_size : (h + 1) * head_size
            ]
    for i in range(tokens):
        score_rows[i * heads : (i + 1) * heads, :] = lax.dot_general(
            q_rows[i * heads : (i + 1) * heads, :].astype(bf16),
            keys[i],
            (((1,), (1,)), ((), ())),
            preferred_element_type=f32,
        )
    blocks = cache_len // 128
    keeps, takes, seen = [], [], []
    position = lax.broadcasted_iota(jnp.int32, (rows, 128), 1)
    for c in range(blocks):
        score = score_rows[:, c * 128 : (c + 1) * 128] * head_size ** (-0.5) + bias
        visible = position + c * 128 < length
        soft = jnp.log1p(jnp.exp(-jnp.abs(score)))
        keeps.append(jnp.where(visible, -jnp.maximum(score, 0.0) - soft, 0.0))
        takes.append(jnp.minimum(score, 0.0) - soft)
        seen.append(visible)
    keep = jnp.concatenate(keeps, axis=0)
    high = keep.astype(bf16)
    rest = keep - high.astype(f32)
    middle = rest.astype(bf16)
    low = (rest - middle.astype(f32)).astype(bf16)
    later = (
        jnp.dot(high, above, preferred_element_type=f32)
        + jnp.dot(middle, above, preferred_element_type=f32)
        + jnp.dot(low, above, preferred_element_type=f32)
    )
    tail = jnp.zeros((rows, 1), f32)
    for c in reversed(range(blocks)):
        exponent = takes[c] + later[c * rows : (c + 1) * rows, :] + tail
        weight_rows[:, c * 128 : (c + 1) * 128] = jnp.where(seen[c], jnp.exp(exponent), 0.0)
        tail = tail + jnp.sum(keeps[c], axis=1, keepdims=True)
    loads[4].wait()
    for i in range(tokens):
        head_rows[i * heads : (i + 1) * heads, :] = jnp.dot(
            weight_rows[i * heads : (i + 1) * heads, :].astype(bf16),
            values[i],
            preferred_element_type=f32,
        )
    h_out[...] = head_rows[:rows, :].astype(bf16)
    for k, to in enumerate(partners):
        push(h_out, h_in.at[ep], (to, tp), h_send.at[k], h_recv.at[ep])
    pltpu.make_async_copy(h_out, h_in.at[ep], h_recv.at[ep]).start()

    loads[5].wait()
    for e in range(n_ep):
        arrived(h_in.at[e], h_recv.at[e])
        head_rows[e * rows : (e + 1) * rows, :] = h_in[e].astype(f32)
    summed = x_all[...] * (1.0 / n_tp)
    for h in range(heads):
        summed = summed + jnp.dot(
            head_rows[pl.ds(h, total, stride=heads), :].astype(bf16),
            out_w[h * head_size : (h + 1) * head_size, :],
            preferred_element_type=f32,
        )
    picked = jnp.dot(pick, summed.astype(bf16), preferred_element_type=f32)
    for e in range(n_ep):
        a_out[e] = picked[e * n_ep : (e + 1) * n_ep, :].astype(bf16)
    routes = [(to, lax.rem(tp + n_tp - 1 - j, n_tp)) for to in partners for j in range(n_tp)]
    routes += [(ep, lax.rem(tp + j, n_tp)) for j in range(1, n_tp)]
    for index, (to, side) in enumerate(routes):
        push(a_out.at[to], a_in.at[ep, tp], (to, side), a_send.at[index], a_recv.at[ep, tp])
    pltpu.make_async_copy(a_out.at[ep], a_in.at[ep, tp], a_recv.at[ep, tp]).start()

    for e in range(n_ep):
        m_out[e] = summed[e * tokens : (e + 1) * tokens, :].astype(bf16)
    side, place = ep // per_part, lax.rem(ep, per_part)
    for k, to in enumerate(partners):
        push(m_out.at[to], m_in.at[place, tp], (to, side), m_send.at[k], m_recv.at[place, tp])

    own = pltpu.make_async_remote_copy(
        src_ref=m_out.at[ep],
        dst_ref=m_in.at[place, tp],
        send_sem=m_send.at[last],
        recv_sem=m_recv.at[place, tp],
        device_id=(ep, side),
        device_id_type=MESH,
    )

    @pl.when(side != tp)
    def _():
        own.start()

    @pl.when(side == tp)
    def _():
        pltpu.make_async_copy(m_out.at[ep], m_in.at[place, tp], m_recv.at[place, tp]).start()

    for load in (loads[6], loads[8], loads[9], loads[10]):
        load.wait()
    gated = jnp.zeros((n_ep, gate_w.shape[0]), f32)
    upped = jnp.zeros((n_ep, up_w.shape[0]), f32)
    squares = jnp.zeros((n_ep, 1), f32)
    for e in range(n_ep):
        for t in range(n_tp):
            arrived(a_in.at[e, t], a_recv.at[e, t])
        block = a_in[e, 0].astype(f32)
        for t in range(1, n_tp):
            block = block + a_in[e, t].astype(f32)
        block = block.astype(bf16).astype(f32)
        squares = squares + jnp.sum(block * block, axis=1, keepdims=True)
        block = (block * moe_gain[:, e * chunk : (e + 1) * chunk]).astype(bf16)
        gated = gated + lax.dot_general(
            block,
            gate_w[:, e * chunk : (e + 1) * chunk],
            (((1,), (1,)), ((), ())),
            preferred_element_type=f32,
        )
        upped = upped + lax.dot_general(
            block,
            up_w[:, e * chunk : (e + 1) * chunk],
            (((1,), (1,)), ((), ())),
            preferred_element_type=f32,
        )
    scale_two = lax.rsqrt(squares * (1.0 / d_model) + rms_epsilon)
    gated = gated * scale_two
    upped = upped * scale_two
    act = (gated / (1.0 + jnp.exp(-gated)) * upped).astype(bf16)
    for t in range(n_tp):
        down = jnp.dot(act, down_w[:, t * part : (t + 1) * part], preferred_element_type=f32)
        for e in range(n_ep):
            z_out[e, t] = jnp.concatenate(
                [down[e : e + 1, : part // 2], down[e : e + 1, part // 2 :]], axis=0
            ).astype(bf16)
    for index, (to, side_to) in enumerate(routes):
        push(
            z_out.at[to, side_to],
            z_in.at[ep, tp],
            (to, side_to),
            z_send.at[index],
            z_recv.at[ep, tp],
        )
    pltpu.make_async_copy(z_out.at[ep, tp], z_in.at[ep, tp], z_recv.at[ep, tp]).start()

    pieces = []
    for c in range(per_part):
        for t in range(n_tp):
            arrived(m_in.at[c, t], m_recv.at[c, t])
        piece = m_in[c, 0].astype(f32)
        for t in range(1, n_tp):
            piece = piece + m_in[c, t].astype(f32)
        pieces.append(piece.astype(bf16).astype(f32))
    result = jnp.concatenate(pieces, axis=1)
    for e in range(n_ep):
        for t in range(n_tp):
            arrived(z_in.at[e, t], z_recv.at[e, t])
        line = z_in[e, 0].astype(f32)
        for t in range(1, n_tp):
            line = line + z_in[e, t].astype(f32)
        line = jnp.concatenate([line[0:1, :], line[1:2, :]], axis=1)
        result = result + mixing[:, e : e + 1] * line
    mixed[...] = result.astype(bf16)

    for copy in sends:
        copy.wait_send()

    @pl.when(side != tp)
    def _():
        own.wait_send()


def layer(
    hidden,
    attn_gain,
    query_weight,
    head_bias,
    key_cache,
    value_cache,
    lengths,
    out_weight,
    moe_gain,
    route_group,
    route_inner,
    route_weight,
    gate_w,
    up_w,
    down_w,
):
    n_tp = lax.axis_size("tp")
    n_ep = lax.axis_size("ep")
    tokens, d_model = hidden.shape
    _, local_kv, cache_len, head_size = key_cache.shape
    chunk, width = query_weight.shape
    part = d_model // n_tp
    heads = width // head_size
    rows = tokens * heads
    slots = route_inner.shape[1]
    experts = gate_w.shape[0] * n_ep
    fits = (
        gate_w.shape[0] == 1
        and local_kv == 1
        and chunk % 128 == 0
        and part % chunk == 0
        and part % 256 == 0
        and n_ep % 8 == 0
        and n_ep <= 16
        and rows % 16 == 0
        and head_size == 128
        and cache_len % 128 == 0
        and tokens * n_ep <= 128
    )
    if not fits:
        return body(
            hidden,
            attn_gain,
            query_weight,
            head_bias,
            key_cache,
            value_cache,
            lengths,
            out_weight,
            moe_gain,
            route_group,
            route_inner,
            route_weight,
            gate_w,
            up_w,
            down_w,
        )
    group_size = experts // max(2, experts // 32)
    f32, bf16 = jnp.float32, jnp.bfloat16
    hbm = pl.BlockSpec(memory_space=pltpu.HBM)
    vmem = pltpu.VMEM
    dma = pltpu.SemaphoreType.DMA
    everyone = n_ep * n_tp
    return pl.pallas_call(
        functools.partial(kernel, n_ep, n_tp, group_size),
        out_shape=pltpu.VMEM((tokens, part), bf16),
        in_specs=[hbm] * 15,
        out_specs=pl.BlockSpec(memory_space=pltpu.VMEM),
        scratch_shapes=[
            pltpu.SMEM(head_bias.shape, f32),
            pltpu.SMEM(lengths.shape, jnp.int32),
            pltpu.SMEM(route_group.shape, jnp.int32),
            pltpu.SMEM((slots, tokens), jnp.int32),
            vmem(hidden.shape, bf16),
            vmem((1, d_model), f32),
            vmem(query_weight.shape, bf16),
            vmem((tokens, cache_len, head_size), bf16),
            vmem((tokens, cache_len, head_size), bf16),
            vmem(out_weight.shape, bf16),
            vmem((1, d_model), f32),
            vmem((slots, tokens), bf16),
            vmem((gate_w.shape[2], d_model), bf16),
            vmem((up_w.shape[2], d_model), bf16),
            vmem(down_w.shape[1:], bf16),
            dma((15,)),
            vmem((n_ep, tokens, chunk), bf16),
            vmem((1, slots * 128), jnp.int32),
            vmem((n_ep, 1, slots * 128), jnp.int32),
            vmem((n_ep, tokens, width), bf16),
            vmem((n_ep, tokens, width), bf16),
            vmem((rows, head_size), bf16),
            vmem((n_ep, rows, head_size), bf16),
            vmem((n_ep, n_ep, chunk), bf16),
            vmem((n_ep, n_tp, n_ep, chunk), bf16),
            vmem((n_ep, tokens, chunk), bf16),
            vmem((part // chunk, n_tp, tokens, chunk), bf16),
            vmem((n_ep, n_tp, 2, part // 2), bf16),
            vmem((n_ep, n_tp, 2, part // 2), bf16),
            dma((n_ep,)),
            dma((n_ep,)),
            dma((n_ep,)),
            dma((n_ep,)),
            dma((n_ep,)),
            dma((n_ep,)),
            dma((n_ep,)),
            dma((n_ep,)),
            dma((everyone,)),
            dma((n_ep, n_tp)),
            dma((n_ep,)),
            dma((part // chunk, n_tp)),
            dma((everyone,)),
            dma((n_ep, n_tp)),
            vmem((tokens * n_ep, chunk), f32),
            vmem((slots, n_ep, 128), jnp.int32),
            vmem((rows, head_size), f32),
            vmem((rows, cache_len), f32),
            vmem((rows, cache_len), f32),
            vmem((rows * n_ep, head_size), f32),
        ],
        compiler_params=pltpu.CompilerParams(
            collective_id=0, has_side_effects=True, vmem_limit_bytes=60 * 1024 * 1024
        ),
    )(
        head_bias,
        lengths,
        route_group,
        route_inner.T,
        hidden,
        attn_gain.reshape(1, d_model),
        query_weight,
        key_cache,
        value_cache,
        out_weight,
        moe_gain.reshape(1, d_model),
        route_weight.T,
        gate_w.swapaxes(1, 2),
        up_w.swapaxes(1, 2),
        down_w,
    )


def solution(mesh):
    placed = (
        P("ep", None),
        P(),
        P("ep", "tp"),
        P(),
        P("ep", "tp", None, None),
        P("ep", "tp", None, None),
        P("ep"),
        P("tp", "ep"),
        P(),
        P("ep"),
        P("ep", None),
        P("ep", None),
        P("ep", None, "tp"),
        P("ep", None, "tp"),
        P("ep", "tp", None),
    )
    return jax.shard_map(layer, mesh=mesh, in_specs=placed, out_specs=P("ep", "tp"), check_vma=False)
```

```python
import functools

import jax
import jax.numpy as jnp
from jax import lax
from jax.experimental import pallas as pl
from jax.experimental.pallas import tpu as pltpu
from jax.sharding import PartitionSpec as P

rms_epsilon = 1e-06


def rms_scale(values, gain):
    wide = values.astype(jnp.float32)
    scaled = wide * lax.rsqrt(jnp.mean(wide * wide, axis=-1, keepdims=True) + rms_epsilon)
    return (scaled * gain).astype(jnp.bfloat16)


def body(
    hidden,
    attn_gain,
    query_weight,
    head_bias,
    key_cache,
    value_cache,
    lengths,
    out_weight,
    moe_gain,
    route_group,
    route_inner,
    route_weight,
    gate_w,
    up_w,
    down_w,
):
    n_tp = lax.axis_size("tp")
    n_ep = lax.axis_size("ep")
    tokens = hidden.shape[0]
    d_model = hidden.shape[1]
    normed = rms_scale(hidden, attn_gain)
    feature_block = lax.all_to_all(normed, "ep", split_axis=1, concat_axis=0, tiled=True)
    queries = lax.psum_scatter(
        jnp.dot(feature_block, query_weight, preferred_element_type=jnp.float32),
        "ep",
        scatter_dimension=0,
        tiled=True,
    ).astype(jnp.bfloat16)
    head_size = key_cache.shape[3]
    local_kv = key_cache.shape[1]
    cache_len = key_cache.shape[2]
    local_heads = queries.shape[1] // head_size
    group_heads = local_heads // local_kv
    queries = queries.reshape(tokens, local_kv, group_heads, head_size)
    own_bias = lax.dynamic_slice_in_dim(
        head_bias, lax.axis_index("tp") * local_heads, local_heads, 0
    )
    own_bias = own_bias.reshape(local_kv, group_heads)
    scores = jnp.einsum(
        "tkgd,tkpd->tkgp", queries, key_cache, preferred_element_type=jnp.float32
    ) * head_size ** (-0.5)
    scores = scores + own_bias[None, :, :, None]
    position = jnp.arange(cache_len, dtype=jnp.int32)
    visible = position[None, None, None, :] < lengths[:, None, None, None]
    log_keep = jnp.where(visible, jax.nn.log_sigmoid(-scores), 0.0)
    later_sum = lax.cumsum(log_keep, axis=3, reverse=True) - log_keep
    weight = jnp.where(visible, jnp.exp(jax.nn.log_sigmoid(scores) + later_sum), 0.0).astype(
        jnp.bfloat16
    )
    heads_out = jnp.einsum(
        "tkgp,tkpd->tkgd", weight, value_cache, preferred_element_type=jnp.float32
    )
    heads_out = heads_out.astype(jnp.bfloat16).reshape(tokens, -1)
    partial_value = jnp.dot(
        heads_out,
        lax.all_gather(out_weight, "ep", axis=1, tiled=True),
        preferred_element_type=jnp.float32,
    )
    rounded = lax.optimization_barrier(partial_value.astype(jnp.bfloat16)).astype(jnp.float32)
    attended = lax.psum(rounded.astype(jnp.bfloat16), "tp").astype(jnp.float32)
    residual = (hidden.astype(jnp.float32) + attended).astype(jnp.bfloat16)
    normed_two = rms_scale(residual, moe_gain)
    per_device = gate_w.shape[0]
    experts = per_device * n_ep
    group_count = max(2, experts // 32)
    group_size = experts // group_count
    chosen = route_group[:, None] * group_size + route_inner
    matches = chosen[:, :, None] == jnp.arange(experts, dtype=jnp.int32)[None, None, :]
    picked = jnp.any(matches, axis=1).astype(jnp.bfloat16)
    mixing = jnp.sum(
        jnp.where(matches, route_weight[:, :, None].astype(jnp.float32), 0.0), axis=1
    ).astype(jnp.bfloat16)
    part_width = d_model // n_tp
    outgoing = jnp.einsum("te,td->ed", picked, normed_two, preferred_element_type=jnp.float32)
    outgoing = outgoing.astype(jnp.bfloat16).reshape(n_ep, per_device, d_model)
    arrived = lax.all_to_all(outgoing, "ep", split_axis=0, concat_axis=0, tiled=True)
    gated_in = jnp.einsum("sed,edf->sef", arrived, gate_w, preferred_element_type=jnp.float32)
    up_proj = jnp.einsum("sed,edf->sef", arrived, up_w, preferred_element_type=jnp.float32)
    activated = (jax.nn.silu(gated_in) * up_proj).astype(jnp.bfloat16)
    down_out = jnp.einsum("sef,efd->sed", activated, down_w, preferred_element_type=jnp.float32)
    down_rounded = lax.optimization_barrier(down_out.astype(jnp.bfloat16)).astype(jnp.float32)
    summed = lax.psum_scatter(
        down_rounded.astype(jnp.bfloat16), "tp", scatter_dimension=2, tiled=True
    )
    returned = lax.all_to_all(summed, "ep", split_axis=0, concat_axis=0, tiled=True).reshape(
        experts, part_width
    )
    routed = jnp.dot(mixing, returned, preferred_element_type=jnp.float32)
    own_residual = lax.dynamic_slice_in_dim(
        residual, lax.axis_index("tp") * part_width, part_width, 1
    )
    return (own_residual.astype(jnp.float32) + routed).astype(jnp.bfloat16)


MESH = pl.DeviceIdType.MESH


def kernel(
    n_ep,
    n_tp,
    group_size,
    head_bias_hbm,
    lengths_hbm,
    route_group_hbm,
    route_inner_hbm,
    hidden_hbm,
    attn_gain_hbm,
    query_hbm,
    key_hbm,
    value_hbm,
    out_hbm,
    moe_gain_hbm,
    route_weight_hbm,
    gate_hbm,
    up_hbm,
    down_hbm,
    mixed,
    head_bias,
    lengths,
    route_group,
    route_inner,
    hidden,
    attn_gain,
    query_w,
    keys,
    values,
    out_w,
    moe_gain,
    route_weight,
    gate_w,
    up_w,
    down_w,
    load_sem,
    x_in,
    r_out,
    r_in,
    q_out,
    q_in,
    h_out,
    h_in,
    a_out,
    a_in,
    m_out,
    m_in,
    z_out,
    z_in,
    x_send,
    x_recv,
    r_send,
    r_recv,
    q_send,
    q_recv,
    h_send,
    h_recv,
    a_send,
    a_recv,
    m_send,
    m_recv,
    z_send,
    z_recv,
    x_all,
    route_all,
    q_rows,
    score_rows,
    weight_rows,
    head_rows,
):
    f32, bf16 = jnp.float32, jnp.bfloat16
    ep = lax.axis_index("ep")
    tp = lax.axis_index("tp")
    tokens, d_model = hidden.shape
    chunk = d_model // n_ep
    total = tokens * n_ep
    cache_len, head_size = keys.shape[1], keys.shape[2]
    heads = query_w.shape[1] // head_size
    rows = tokens * heads
    part = d_model // n_tp
    per_part = part // chunk
    slots = route_inner.shape[0]

    loads = [
        pltpu.make_async_copy(src, dst, load_sem.at[index])
        for index, (src, dst) in enumerate(
            (
                (hidden_hbm, hidden),
                (attn_gain_hbm, attn_gain),
                (query_hbm, query_w),
                (key_hbm.at[:, 0], keys),
                (value_hbm.at[:, 0], values),
                (out_hbm, out_w),
                (moe_gain_hbm, moe_gain),
                (route_weight_hbm, route_weight),
                (gate_hbm.at[0], gate_w),
                (up_hbm.at[0], up_w),
                (down_hbm.at[0], down_w),
                (route_group_hbm, route_group),
                (route_inner_hbm, route_inner),
                (lengths_hbm, lengths),
                (head_bias_hbm, head_bias),
            )
        )
    ]
    loads[0].start()

    barrier = pltpu.get_barrier_semaphore()
    others = [(i, 0) for i in range(1, n_ep)] + [(0, j) for j in range(1, n_tp)]
    for i, j in others:
        peer = (lax.rem(ep + i, n_ep), lax.rem(tp + j, n_tp))
        pl.semaphore_signal(barrier, inc=1, device_id=peer, device_id_type=MESH)

    for load in loads[11:13] + loads[1:11] + loads[13:]:
        load.start()

    loads[11].wait()
    loads[12].wait()
    lane = lax.broadcasted_iota(jnp.int32, (1, slots * 128), 1)
    own_route = jnp.full((1, slots * 128), -1, jnp.int32)
    chosen = [
        [route_group[i] * group_size + route_inner[k, i] for k in range(slots)]
        for i in range(tokens)
    ]
    for i in range(tokens):
        for k in range(slots):
            own_route = jnp.where(lane == k * 128 + ep * tokens + i, chosen[i][k], own_route)
    r_out[...] = own_route

    pl.semaphore_wait(barrier, len(others))
    loads[0].wait()

    sends = []
    last = n_ep - 1
    upper = ep >= n_ep // 2

    def partner(step):
        down_to = last - step - jnp.where(last - step <= ep, 1, 0)
        up_to = step + jnp.where(step >= ep, 1, 0)
        return jnp.where(upper, up_to, down_to)

    partners = [partner(step) for step in range(last)]

    def push(src, dst, peer, send_sem, recv_sem):
        copy = pltpu.make_async_remote_copy(
            src_ref=src,
            dst_ref=dst,
            send_sem=send_sem,
            recv_sem=recv_sem,
            device_id=peer,
            device_id_type=MESH,
        )
        copy.start()
        sends.append(copy)

    def arrived(ref, sem):
        pltpu.make_async_copy(ref, ref, sem).wait()

    def columns(index, width):
        return pl.ds(pl.multiple_of(index * width, 128), width)

    for k, to in enumerate(partners):
        push(hidden.at[:, columns(to, chunk)], x_in.at[ep], (to, tp), x_send.at[k], x_recv.at[ep])
    pltpu.make_async_copy(hidden.at[:, columns(ep, chunk)], x_in.at[ep], x_recv.at[ep]).start()
    for k, to in enumerate(partners):
        push(r_out, r_in.at[ep], (to, tp), r_send.at[k], r_recv.at[ep])
    pltpu.make_async_copy(r_out, r_in.at[ep], r_recv.at[ep]).start()

    wide = hidden[...].astype(f32)
    scale = lax.rsqrt(jnp.mean(wide * wide, axis=-1, keepdims=True) + rms_epsilon)

    loads[7].wait()
    shares = route_weight[...].astype(f32)
    token = lax.broadcasted_iota(jnp.int32, (tokens, 128), 0)
    expert = lax.broadcasted_iota(jnp.int32, (tokens, 128), 1)
    mixing = jnp.zeros((tokens, 128), f32)
    for k in range(slots):
        for i in range(tokens):
            mixing = mixing + jnp.where(
                (token == i) & (expert == chosen[i][k]), shares[k : k + 1, i : i + 1], 0.0
            )

    loads[1].wait()
    loads[2].wait()
    for e in range(n_ep):
        arrived(x_in.at[e], x_recv.at[e])
        x_all[e * tokens : (e + 1) * tokens, :] = x_in[e].astype(f32)
    features = (x_all[...] * attn_gain[:, columns(ep, chunk)]).astype(bf16)
    query_parts = jnp.dot(features, query_w[...], preferred_element_type=f32)
    for e in range(n_ep):
        q_out[e] = query_parts[e * tokens : (e + 1) * tokens, :].astype(bf16)
    for k, to in enumerate(partners):
        push(q_out.at[to], q_in.at[ep], (to, tp), q_send.at[k], q_recv.at[ep])
    pltpu.make_async_copy(q_out.at[ep], q_in.at[ep], q_recv.at[ep]).start()

    for e in range(n_ep):
        arrived(r_in.at[e], r_recv.at[e])
        for k in range(slots):
            route_all[k, e : e + 1, :] = r_in[e, :, k * 128 : (k + 1) * 128]
    tables = [route_all[k] for k in range(slots)]
    picks = []
    for e in range(n_ep):
        hit = tables[0] == e
        for table in tables[1:]:
            hit = hit | (table == e)
        picks.append(jnp.where(hit, 1.0, 0.0))
    pick = jnp.concatenate(picks, axis=0)[:, :total].astype(bf16)

    loads[13].wait()
    loads[14].wait()
    row = lax.broadcasted_iota(jnp.int32, (rows, 1), 0)
    bias = jnp.zeros((rows, 1), f32)
    length = jnp.zeros((rows, 1), jnp.int32)
    for i in range(tokens):
        length = jnp.where(row // heads == i, lengths[i], length)
    for h in range(heads):
        bias = jnp.where(row % heads == h, head_bias[tp * heads + h], bias)
    above = lax.broadcasted_iota(jnp.int32, (128, 128), 0) > lax.broadcasted_iota(
        jnp.int32, (128, 128), 1
    )
    above = jnp.where(above, 1.0, 0.0).astype(bf16)
    loads[3].wait()

    for e in range(n_ep):
        arrived(q_in.at[e], q_recv.at[e])
    queries = q_in[0].astype(f32)
    for e in range(1, n_ep):
        queries = queries + q_in[e].astype(f32)
    queries = queries * scale
    for i in range(tokens):
        for h in range(heads):
            q_rows[i * heads + h : i * heads + h + 1, :] = queries[
                i : i + 1, h * head_size : (h + 1) * head_size
            ]
    for i in range(tokens):
        score_rows[i * heads : (i + 1) * heads, :] = lax.dot_general(
            q_rows[i * heads : (i + 1) * heads, :].astype(bf16),
            keys[i],
            (((1,), (1,)), ((), ())),
            preferred_element_type=f32,
        )
    blocks = cache_len // 128
    keeps, takes, seen = [], [], []
    position = lax.broadcasted_iota(jnp.int32, (rows, 128), 1)
    for c in range(blocks):
        score = score_rows[:, c * 128 : (c + 1) * 128] * head_size ** (-0.5) + bias
        visible = position + c * 128 < length
        soft = jnp.log1p(jnp.exp(-jnp.abs(score)))
        keeps.append(jnp.where(visible, -jnp.maximum(score, 0.0) - soft, 0.0))
        takes.append(jnp.minimum(score, 0.0) - soft)
        seen.append(visible)
    keep = jnp.concatenate(keeps, axis=0)
    high = keep.astype(bf16)
    rest = keep - high.astype(f32)
    middle = rest.astype(bf16)
    low = (rest - middle.astype(f32)).astype(bf16)
    later = (
        jnp.dot(high, above, preferred_element_type=f32)
        + jnp.dot(middle, above, preferred_element_type=f32)
        + jnp.dot(low, above, preferred_element_type=f32)
    )
    tail = jnp.zeros((rows, 1), f32)
    for c in reversed(range(blocks)):
        exponent = takes[c] + later[c * rows : (c + 1) * rows, :] + tail
        weight_rows[:, c * 128 : (c + 1) * 128] = jnp.where(seen[c], jnp.exp(exponent), 0.0)
        tail = tail + jnp.sum(keeps[c], axis=1, keepdims=True)
    loads[4].wait()
    for i in range(tokens):
        head_rows[i * heads : (i + 1) * heads, :] = jnp.dot(
            weight_rows[i * heads : (i + 1) * heads, :].astype(bf16),
            values[i],
            preferred_element_type=f32,
        )
    h_out[...] = head_rows[:rows, :].astype(bf16)
    for k, to in enumerate(partners):
        push(h_out, h_in.at[ep], (to, tp), h_send.at[k], h_recv.at[ep])
    pltpu.make_async_copy(h_out, h_in.at[ep], h_recv.at[ep]).start()

    loads[5].wait()
    for e in range(n_ep):
        arrived(h_in.at[e], h_recv.at[e])
        head_rows[e * rows : (e + 1) * rows, :] = h_in[e].astype(f32)
    summed = x_all[...] * (1.0 / n_tp)
    for h in range(heads):
        summed = summed + jnp.dot(
            head_rows[pl.ds(h, total, stride=heads), :].astype(bf16),
            out_w[h * head_size : (h + 1) * head_size, :],
            preferred_element_type=f32,
        )
    picked = jnp.dot(pick, summed.astype(bf16), preferred_element_type=f32)
    for e in range(n_ep):
        a_out[e] = picked[e * n_ep : (e + 1) * n_ep, :].astype(bf16)
    routes = [(to, lax.rem(tp + n_tp - 1 - j, n_tp)) for to in partners for j in range(n_tp)]
    routes += [(ep, lax.rem(tp + j, n_tp)) for j in range(1, n_tp)]
    for index, (to, side) in enumerate(routes):
        push(a_out.at[to], a_in.at[ep, tp], (to, side), a_send.at[index], a_recv.at[ep, tp])
    pltpu.make_async_copy(a_out.at[ep], a_in.at[ep, tp], a_recv.at[ep, tp]).start()

    for e in range(n_ep):
        m_out[e] = summed[e * tokens : (e + 1) * tokens, :].astype(bf16)
    side, place = ep // per_part, lax.rem(ep, per_part)
    for k, to in enumerate(partners):
        push(m_out.at[to], m_in.at[place, tp], (to, side), m_send.at[k], m_recv.at[place, tp])

    own = pltpu.make_async_remote_copy(
        src_ref=m_out.at[ep],
        dst_ref=m_in.at[place, tp],
        send_sem=m_send.at[last],
        recv_sem=m_recv.at[place, tp],
        device_id=(ep, side),
        device_id_type=MESH,
    )

    @pl.when(side != tp)
    def _():
        own.start()

    @pl.when(side == tp)
    def _():
        pltpu.make_async_copy(m_out.at[ep], m_in.at[place, tp], m_recv.at[place, tp]).start()

    for load in (loads[6], loads[8], loads[9], loads[10]):
        load.wait()
    gated = jnp.zeros((n_ep, gate_w.shape[0]), f32)
    upped = jnp.zeros((n_ep, up_w.shape[0]), f32)
    squares = jnp.zeros((n_ep, 1), f32)
    for e in range(n_ep):
        for t in range(n_tp):
            arrived(a_in.at[e, t], a_recv.at[e, t])
        block = a_in[e, 0].astype(f32)
        for t in range(1, n_tp):
            block = block + a_in[e, t].astype(f32)
        block = block.astype(bf16).astype(f32)
        squares = squares + jnp.sum(block * block, axis=1, keepdims=True)
        block = (block * moe_gain[:, e * chunk : (e + 1) * chunk]).astype(bf16)
        gated = gated + lax.dot_general(
            block,
            gate_w[:, e * chunk : (e + 1) * chunk],
            (((1,), (1,)), ((), ())),
            preferred_element_type=f32,
        )
        upped = upped + lax.dot_general(
            block,
            up_w[:, e * chunk : (e + 1) * chunk],
            (((1,), (1,)), ((), ())),
            preferred_element_type=f32,
        )
    scale_two = lax.rsqrt(squares * (1.0 / d_model) + rms_epsilon)
    gated = gated * scale_two
    upped = upped * scale_two
    act = (gated / (1.0 + jnp.exp(-gated)) * upped).astype(bf16)
    for t in range(n_tp):
        down = jnp.dot(act, down_w[:, t * part : (t + 1) * part], preferred_element_type=f32)
        for e in range(n_ep):
            z_out[e, t] = jnp.concatenate(
                [down[e : e + 1, : part // 2], down[e : e + 1, part // 2 :]], axis=0
            ).astype(bf16)
    for index, (to, side_to) in enumerate(routes):
        push(
            z_out.at[to, side_to],
            z_in.at[ep, tp],
            (to, side_to),
            z_send.at[index],
            z_recv.at[ep, tp],
        )
    pltpu.make_async_copy(z_out.at[ep, tp], z_in.at[ep, tp], z_recv.at[ep, tp]).start()

    pieces = []
    for c in range(per_part):
        for t in range(n_tp):
            arrived(m_in.at[c, t], m_recv.at[c, t])
        piece = m_in[c, 0].astype(f32)
        for t in range(1, n_tp):
            piece = piece + m_in[c, t].astype(f32)
        pieces.append(piece.astype(bf16).astype(f32))
    result = jnp.concatenate(pieces, axis=1)
    for e in range(n_ep):
        for t in range(n_tp):
            arrived(z_in.at[e, t], z_recv.at[e, t])
        line = z_in[e, 0].astype(f32)
        for t in range(1, n_tp):
            line = line + z_in[e, t].astype(f32)
        line = jnp.concatenate([line[0:1, :], line[1:2, :]], axis=1)
        result = result + mixing[:, e : e + 1] * line
    mixed[...] = result.astype(bf16)

    for copy in sends:
        copy.wait_send()

    @pl.when(side != tp)
    def _():
        own.wait_send()


def layer(
    hidden,
    attn_gain,
    query_weight,
    head_bias,
    key_cache,
    value_cache,
    lengths,
    out_weight,
    moe_gain,
    route_group,
    route_inner,
    route_weight,
    gate_w,
    up_w,
    down_w,
):
    n_tp = lax.axis_size("tp")
    n_ep = lax.axis_size("ep")
    tokens, d_model = hidden.shape
    _, local_kv, cache_len, head_size = key_cache.shape
    chunk, width = query_weight.shape
    part = d_model // n_tp
    heads = width // head_size
    rows = tokens * heads
    slots = route_inner.shape[1]
    experts = gate_w.shape[0] * n_ep
    fits = (
        gate_w.shape[0] == 1
        and local_kv == 1
        and chunk % 128 == 0
        and part % chunk == 0
        and part % 256 == 0
        and n_ep % 8 == 0
        and n_ep <= 16
        and rows % 16 == 0
        and head_size == 128
        and cache_len % 128 == 0
        and tokens * n_ep <= 128
    )
    if not fits:
        return body(
            hidden,
            attn_gain,
            query_weight,
            head_bias,
            key_cache,
            value_cache,
            lengths,
            out_weight,
            moe_gain,
            route_group,
            route_inner,
            route_weight,
            gate_w,
            up_w,
            down_w,
        )
    group_size = experts // max(2, experts // 32)
    f32, bf16 = jnp.float32, jnp.bfloat16
    hbm = pl.BlockSpec(memory_space=pltpu.HBM)
    vmem = pltpu.VMEM
    dma = pltpu.SemaphoreType.DMA
    everyone = n_ep * n_tp
    return pl.pallas_call(
        functools.partial(kernel, n_ep, n_tp, group_size),
        out_shape=pltpu.VMEM((tokens, part), bf16),
        in_specs=[hbm] * 15,
        out_specs=pl.BlockSpec(memory_space=pltpu.VMEM),
        scratch_shapes=[
            pltpu.SMEM(head_bias.shape, f32),
            pltpu.SMEM(lengths.shape, jnp.int32),
            pltpu.SMEM(route_group.shape, jnp.int32),
            pltpu.SMEM((slots, tokens), jnp.int32),
            vmem(hidden.shape, bf16),
            vmem((1, d_model), f32),
            vmem(query_weight.shape, bf16),
            vmem((tokens, cache_len, head_size), bf16),
            vmem((tokens, cache_len, head_size), bf16),
            vmem(out_weight.shape, bf16),
            vmem((1, d_model), f32),
            vmem((slots, tokens), bf16),
            vmem((gate_w.shape[2], d_model), bf16),
            vmem((up_w.shape[2], d_model), bf16),
            vmem(down_w.shape[1:], bf16),
            dma((15,)),
            vmem((n_ep, tokens, chunk), bf16),
            vmem((1, slots * 128), jnp.int32),
            vmem((n_ep, 1, slots * 128), jnp.int32),
            vmem((n_ep, tokens, width), bf16),
            vmem((n_ep, tokens, width), bf16),
            vmem((rows, head_size), bf16),
            vmem((n_ep, rows, head_size), bf16),
            vmem((n_ep, n_ep, chunk), bf16),
            vmem((n_ep, n_tp, n_ep, chunk), bf16),
            vmem((n_ep, tokens, chunk), bf16),
            vmem((part // chunk, n_tp, tokens, chunk), bf16),
            vmem((n_ep, n_tp, 2, part // 2), bf16),
            vmem((n_ep, n_tp, 2, part // 2), bf16),
            dma((n_ep,)),
            dma((n_ep,)),
            dma((n_ep,)),
            dma((n_ep,)),
            dma((n_ep,)),
            dma((n_ep,)),
            dma((n_ep,)),
            dma((n_ep,)),
            dma((everyone,)),
            dma((n_ep, n_tp)),
            dma((n_ep,)),
            dma((part // chunk, n_tp)),
            dma((everyone,)),
            dma((n_ep, n_tp)),
            vmem((tokens * n_ep, chunk), f32),
            vmem((slots, n_ep, 128), jnp.int32),
            vmem((rows, head_size), f32),
            vmem((rows, cache_len), f32),
            vmem((rows, cache_len), f32),
            vmem((rows * n_ep, head_size), f32),
        ],
        compiler_params=pltpu.CompilerParams(
            collective_id=0, has_side_effects=True, vmem_limit_bytes=60 * 1024 * 1024
        ),
    )(
        head_bias,
        lengths,
        route_group,
        route_inner.T,
        hidden,
        attn_gain.reshape(1, d_model),
        query_weight,
        key_cache,
        value_cache,
        out_weight,
        moe_gain.reshape(1, d_model),
        route_weight.T,
        gate_w.swapaxes(1, 2),
        up_w.swapaxes(1, 2),
        down_w,
    )


def solution(mesh):
    placed = (
        P("ep", None),
        P(),
        P("ep", "tp"),
        P(),
        P("ep", "tp", None, None),
        P("ep", "tp", None, None),
        P("ep"),
        P("tp", "ep"),
        P(),
        P("ep"),
        P("ep", None),
        P("ep", None),
        P("ep", None, "tp"),
        P("ep", None, "tp"),
        P("ep", "tp", None),
    )
    return jax.shard_map(layer, mesh=mesh, in_specs=placed, out_specs=P("ep", "tp"), check_vma=False)
```
